256 devices in a mesh: grp: 2 (over y), fs: 16 (over z), tp: 8 (over x, core).
Axes of the slice: x: 4, y: 2, z: 16, core: 2. Of those that a mesh axis runs over, the one named last changes fastest.
The devices are a block of a 4x16x16 slice.
Arguments:
- incoming_representations: bfloat16 [20480, 2048], P(('grp', 'fs', 'tp')), parts along dimension 0, may hold values from -6 to 6
- perceptron_switch_coefficients: bfloat16 [2048, 5120], P('fs', 'tp'), may hold values from -0.125 to 0.125
- perceptron_expand_coefficients: bfloat16 [2048, 5120], P('fs', 'tp'), may hold values from -0.125 to 0.125
- perceptron_contract_coefficients: bfloat16 [5120, 2048], P('tp', 'fs'), may hold values from -0.5 to 0.5
- probe_coefficients: bfloat16 [2048, 512], P('fs', 'tp'), may hold values from -0.125 to 0.125
- address_coefficients: bfloat16 [2048, 512], P('fs', 'tp'), may hold values from -0.125 to 0.125
- payload_coefficients: bfloat16 [2048, 1024], P('fs', 'tp'), may hold values from -0.125 to 0.125
- emit_switch_coefficients: bfloat16 [2048, 1024], P('fs', 'tp'), may hold values from -0.125 to 0.125
- forgetting_shrink_coefficients: bfloat16 [2048, 32], replicated, may hold values from -0.125 to 0.125
- forgetting_expand_coefficients: bfloat16 [32, 512], P(None, 'tp'), may hold values from -3 to 3
- forgetting_sigmoid_intercept: float32 [512], P('tp'), may hold values from -1 to 9
- extra_forgetting_logits: float32 [20480, 512], P(('grp', 'fs'), 'tp'), parts along dimension 0, may hold values from -0.7 to 0
- subspace_rescaling_amplitude: float32 [128], replicated, may hold values from 0.1 to 1.9
- recurrence_emit_coefficients: bfloat16 [1024, 2048], P('tp', 'fs'), may hold values from -0.5 to 0.5
Outputs:
- layer_out: bfloat16 [20480, 2048], P(('grp', 'fs', 'tp')), parts along dimension 0
The draws below stay inside these ranges and needn't reach their ends.
There are 2 independent parts, one for each index of `grp`. The reference program is written for one: setup_inputs(seed, part) draws one part's arguments, and reference() takes and returns one part's arrays. A program takes and returns all parts, laid end to end along the dimension named above; an argument that names none is the same for every part. Nothing has to cross between parts.
All inputs are finite; a program needn't handle non-finite values.
Results may differ from the reference program's by a relative error of at most 0.035.
Values may be sent and summed in bfloat16 or wider, within the bound.
A program may use at most 64 MiB of HBM per device.

```python
import math
import jax
import jax.numpy as jnp
from jax import lax

D = 2048
FF = 5120
HEADS = 8
DK = 64
DV = 128
RANK = 32
BLOCK = 64
SEQUENCE_LENGTH = 320
TOKEN_TOTAL = 10240
N_TP = 8


def draw_forgetting_sigmoid_intercept(key, part):
    channels = HEADS * DK
    sequence_streams = jax.random.split(jax.random.fold_in(key, 7), 3)
    percent = 50
    chosen = (jax.random.randint(sequence_streams[0], (channels,), 0, 100) < percent).astype(jnp.float32)
    fast_bias = jax.random.uniform(sequence_streams[1], (channels,), jnp.float32, -1.0, 0.8)
    slow_bias = jax.random.uniform(sequence_streams[2], (channels,), jnp.float32, 5.0, 9.0)
    return chosen * fast_bias + (1.0 - chosen) * slow_bias


def draw_extra_forgetting_logits(key, part):
    channels = HEADS * DK
    sequence_streams = jax.random.split(jax.random.fold_in(key, 11), 4)
    sequence_total = TOKEN_TOTAL // SEQUENCE_LENGTH
    spike_first = jax.random.randint(sequence_streams[0], (sequence_total, 1), 0, SEQUENCE_LENGTH)
    spike_second = jax.random.randint(sequence_streams[1], (sequence_total, 1), 0, SEQUENCE_LENGTH)
    token_positions = jnp.arange(SEQUENCE_LENGTH)[None, :]
    spike_mask = ((token_positions == spike_first) | (token_positions == spike_second)).astype(jnp.float32).reshape(TOKEN_TOTAL, 1)
    spike_strength = jax.random.uniform(sequence_streams[2], (TOKEN_TOTAL, channels), jnp.float32, 0.22, 0.69)
    block_total = TOKEN_TOTAL // BLOCK
    decay_offset_term = jnp.exp(jax.random.uniform(sequence_streams[3], (block_total, 1, channels), jnp.float32, math.log(0.0002), math.log(0.003)))
    decay_offset_term = jnp.broadcast_to(decay_offset_term, (block_total, BLOCK, channels)).reshape(TOKEN_TOTAL, channels)
    return -(spike_mask * spike_strength + decay_offset_term)


def block_scale(own_key, shape, pieces, low, largest):
    gain = 1.0
    for position, parts in pieces:
        heights = jax.random.uniform(jax.random.fold_in(jax.random.fold_in(own_key, 6), position), (parts,), jnp.float32, low / len(pieces), largest / len(pieces))
        gain = gain * jnp.repeat(jnp.exp(heights), shape[position] // parts).reshape((-1,) + (1,) * (len(shape) - 1 - position))
    return gain


def bell_draw(stream_key, shape, width, limit, pieces=(), kind=jnp.bfloat16):
    loudness = block_scale(stream_key, shape, pieces, -0.22, 0.18) if pieces else 1.0
    values = jax.random.normal(stream_key, shape, jnp.float32) * width * loudness
    return jnp.minimum(jnp.maximum(values, -limit), limit).astype(kind)


def setup_inputs(seed: int = 0, part: int = 0) -> dict:
    seeds = jax.random.split(jax.random.key(seed), 15)
    part_splits = jax.random.split(jax.random.fold_in(seeds[14], part), 15)
    return {
        "incoming_representations": bell_draw(part_splits[0], (TOKEN_TOTAL, D), 1.0, 6.0, ((0, 128),)),
        "perceptron_switch_coefficients": bell_draw(seeds[1], (D, FF), D ** -0.5, 0.125, ((0, 16), (1, 8))),
        "perceptron_expand_coefficients": bell_draw(seeds[2], (D, FF), D ** -0.5, 0.125, ((0, 16), (1, 8))),
        "perceptron_contract_coefficients": bell_draw(seeds[3], (FF, D), (max(FF // 36, 1)) ** -0.5, 0.5, ((0, 8), (1, 16))),
        "probe_coefficients": bell_draw(seeds[4], (D, HEADS * DK), D ** -0.5, 0.125, ((0, 16), (1, 8))),
        "address_coefficients": bell_draw(seeds[5], (D, HEADS * DK), D ** -0.5, 0.125, ((0, 16), (1, 8))),
        "payload_coefficients": bell_draw(seeds[6], (D, HEADS * DV), D ** -0.5, 0.125, ((0, 16), (1, 8))),
        "emit_switch_coefficients": bell_draw(seeds[7], (D, HEADS * DV), D ** -0.5, 0.125, ((0, 16), (1, 8))),
        "forgetting_shrink_coefficients": bell_draw(seeds[8], (D, RANK), D ** -0.5, 0.125),
        "forgetting_expand_coefficients": bell_draw(seeds[9], (RANK, HEADS * DK), (3 * RANK ** -0.5), 3.0, ((1, 8),)),
        "forgetting_sigmoid_intercept": draw_forgetting_sigmoid_intercept(jax.random.fold_in(seeds[14], 71), part),
        "extra_forgetting_logits": draw_extra_forgetting_logits(jax.random.fold_in(jax.random.fold_in(seeds[14], part), 71), part),
        "subspace_rescaling_amplitude": jnp.clip(1.0 + 0.18 * jax.random.normal(seeds[12], (DV,), jnp.float32), 0.1, 1.9),
        "recurrence_emit_coefficients": bell_draw(seeds[13], (HEADS * DV, D), (max(HEADS * DV // 9, 1)) ** -0.5, 0.5, ((0, 8), (1, 16))),
    }


residual_gain = 1.681792830507429
forgetting_steepness_multiplier = 16.0
epsilon = 1e-06
highest = lax.Precision.HIGHEST

def post_norm(residual, branch):
    summed = residual_gain * residual.astype(jnp.float32) + branch
    average = lax.optimization_barrier(jnp.mean(summed, axis=-1, keepdims=True))
    centred = summed - average
    variance = lax.optimization_barrier(jnp.mean(centred * centred, axis=-1, keepdims=True))
    return (centred * lax.rsqrt(variance + epsilon)).astype(jnp.bfloat16)

def rounded_sum(hidden, weight):
    block_width = hidden.shape[1] // N_TP
    totals = jnp.zeros((hidden.shape[0], weight.shape[1]), jnp.float32)
    for block_index in range(N_TP):
        begin = block_index * block_width
        partial_value = jnp.dot(hidden[:, begin:begin + block_width], weight[begin:begin + block_width], preferred_element_type=jnp.float32)
        partial_value = lax.optimization_barrier(partial_value.astype(jnp.bfloat16))
        totals = totals + partial_value.astype(jnp.float32)
    return totals

def channel_half(latent_representations, perceptron_switch_coefficients, perceptron_expand_coefficients, perceptron_contract_coefficients):
    gate_sum = jnp.dot(latent_representations, perceptron_switch_coefficients, preferred_element_type=jnp.float32)
    up_sum = jnp.dot(latent_representations, perceptron_expand_coefficients, preferred_element_type=jnp.float32)
    hidden = (jax.nn.silu(gate_sum) * up_sum).astype(jnp.bfloat16)
    return post_norm(latent_representations, 0.5 * rounded_sum(hidden, perceptron_contract_coefficients))

def linear_attention(queries, key_rows, values, forgetting_euler_power):
    token_count = queries.shape[0]
    seq_count = token_count // SEQUENCE_LENGTH

    def by_position(source, channels):
        shaped = source.astype(jnp.float32).reshape(seq_count, SEQUENCE_LENGTH, HEADS, channels)
        return shaped.transpose(1, 0, 2, 3)
    inputs = (by_position(queries, DK), by_position(key_rows, DK), by_position(values, DV), jnp.exp(by_position(forgetting_euler_power, DK)))
    start_state = jnp.zeros((seq_count, HEADS, DK, DV), jnp.float32)

    def forward(carried, step_in):
        query_now, key_now, value_now, decay_now = step_in
        carried = decay_now[..., None] * carried + key_now[..., None] * value_now[..., None, :]
        return (carried, jnp.einsum('shd,shdv->shv', query_now, carried, precision=highest))

    def reverse_direction_sweep(carried, step_in):
        query_now, key_now, value_now, decay_now = step_in
        seen = decay_now[..., None] * carried
        return (seen + key_now[..., None] * value_now[..., None, :], jnp.einsum('shd,shdv->shv', query_now, seen, precision=highest))
    _, from_before = lax.scan(forward, start_state, inputs)
    _, from_after = lax.scan(reverse_direction_sweep, start_state, inputs, reverse=True)
    return (from_before + from_after).transpose(1, 0, 2, 3).reshape(token_count, HEADS, DV)

def recurrent_context_blender(latent_representations, probe_coefficients, address_coefficients, payload_coefficients, emit_switch_coefficients, forgetting_shrink_coefficients, forgetting_expand_coefficients, forgetting_sigmoid_intercept, extra_forgetting_logits, subspace_rescaling_amplitude, recurrence_emit_coefficients):
    queries = jnp.dot(latent_representations, probe_coefficients, preferred_element_type=jnp.float32).astype(jnp.bfloat16)
    key_rows = jnp.dot(latent_representations, address_coefficients, preferred_element_type=jnp.float32).astype(jnp.bfloat16)
    values = jnp.dot(latent_representations, payload_coefficients, preferred_element_type=jnp.float32).astype(jnp.bfloat16)
    outgate = jnp.dot(latent_representations, emit_switch_coefficients, preferred_element_type=jnp.float32).astype(jnp.bfloat16)
    compact_inner_dimensionality = jnp.dot(latent_representations, forgetting_shrink_coefficients, preferred_element_type=jnp.float32).astype(jnp.bfloat16)
    forgetting_euler_power = jax.nn.log_sigmoid(jnp.dot(compact_inner_dimensionality, forgetting_expand_coefficients, preferred_element_type=jnp.float32) + forgetting_sigmoid_intercept) / forgetting_steepness_multiplier + extra_forgetting_logits
    mixed_heads = linear_attention(queries, key_rows, values, forgetting_euler_power)
    scaled = mixed_heads * lax.rsqrt(lax.optimization_barrier(jnp.mean(mixed_heads * mixed_heads, axis=-1, keepdims=True)) + epsilon) * subspace_rescaling_amplitude
    opener = jax.nn.silu(outgate.astype(jnp.float32)).reshape(mixed_heads.shape)
    gated = (scaled * opener).reshape(mixed_heads.shape[0], HEADS * DV).astype(jnp.bfloat16)
    return post_norm(latent_representations, rounded_sum(gated, recurrence_emit_coefficients))

def reference(incoming_representations, perceptron_switch_coefficients, perceptron_expand_coefficients, perceptron_contract_coefficients, probe_coefficients, address_coefficients, payload_coefficients, emit_switch_coefficients, forgetting_shrink_coefficients, forgetting_expand_coefficients, forgetting_sigmoid_intercept, extra_forgetting_logits, subspace_rescaling_amplitude, recurrence_emit_coefficients):
    opening_perceptron_result = channel_half(incoming_representations, perceptron_switch_coefficients, perceptron_expand_coefficients, perceptron_contract_coefficients)
    context_blend_result = recurrent_context_blender(opening_perceptron_result, probe_coefficients, address_coefficients, payload_coefficients, emit_switch_coefficients, forgetting_shrink_coefficients, forgetting_expand_coefficients, forgetting_sigmoid_intercept, extra_forgetting_logits, subspace_rescaling_amplitude, recurrence_emit_coefficients)
    return channel_half(context_blend_result, perceptron_switch_coefficients, perceptron_expand_coefficients, perceptron_contract_coefficients)
```

```python
import functools

import jax
import jax.numpy as jnp
from jax import lax
from jax.experimental import pallas as pl
from jax.experimental.pallas import tpu as pltpu
from jax.sharding import PartitionSpec as P

MESH = pl.DeviceIdType.MESH
DK = 64
DV = 128
SEQ = 320
PAD = 384
GAIN = 1.681792830507429
STEEP = 16.0
EPS = 1e-06
CHUNKS = 2
OFFSETS = (0, 3, 6, 6)
RIGHT, LEFT = 0, 1
A, B = 0, 1
f32, bf16 = jnp.float32, jnp.bfloat16


def mo(v, m):
    return pl.multiple_of(v, m)


def dot(a, b):
    return jnp.dot(a, b, preferred_element_type=f32)


def dot_t(a, b):
    return lax.dot_general(a, b, (((1,), (1,)), ((), ())), preferred_element_type=f32)


def kernel(
    n,
    x_in, wsw, wex, wct, wq, wk, wv, wg, wls, wle, bias, extra, gain, wo,
    out,
    gu, dn, qb, ob, xg, hb, pp, rp, sm, st, rt, br,
    qk, vb, og, lg, mm, wle2, bias2, extra2, gt,
    z_recv, c_recv, z_send, ag_recv, ag_send, rs_recv, rs_send, loc,
):
    T, D = x_in.shape
    K = wsw.shape[0]
    F = wsw.shape[1]
    H = n // 2
    zi = lax.axis_index("fs")
    gi = lax.axis_index("grp")
    ti = lax.axis_index("tp")
    par = lax.rem(gi, 2)
    ci = lax.rem(ti, 2)
    xi = lax.div(ti, 2)
    oc = 1 - ci
    x1 = lax.rem(xi + 1, 4)
    x2 = lax.rem(xi + 2, 4)
    x3 = lax.rem(xi + 3, 4)
    z_right = {"fs": lax.rem(zi + 1, n)}
    z_left = {"fs": lax.rem(zi + n - 1, n)}
    y_dev = {"grp": gi + 1 - 2 * par}
    x_right = {"tp": x1 * 2 + ci}
    x_left = {"tp": x3 * 2 + ci}
    mate = {"tp": xi * 2 + oc}
    z_dev = (z_right, z_left)

    def remote(src, dst, s, r, dev):
        return pltpu.make_async_remote_copy(
            src_ref=src, dst_ref=dst, send_sem=s, recv_sem=r, device_id=dev, device_id_type=MESH
        )

    locals_ = []
    own = pl.ds(mo(zi * K, K), K)
    for j in range(F // 128):
        col = slice(j * 128, j * 128 + 128)
        locals_.append((wsw.at[:, col], gu.at[own, pl.ds(j * 256, 128)]))
        locals_.append((wex.at[:, col], gu.at[own, pl.ds(j * 256 + 128, 128)]))
    locals_.append((x_in, xg.at[0, pl.ds(mo((ci * 4 + xi) * T, 16), T)]))
    locals_.append((wct, dn.at[:, own]))
    locals_.append((wv, qb.at[own, pl.ds(128, 128)]))
    locals_.append((wg, qb.at[own, pl.ds(256, 128)]))
    locals_.append((wo, ob.at[:, own]))
    locals_ = [pltpu.make_async_copy(s, d, loc.at[i]) for i, (s, d) in enumerate(locals_)]
    for c in locals_:
        c.start()
    qb[own, 0:64] = wq[...]
    qb[own, 64:128] = wk[...]

    barrier = pltpu.get_barrier_semaphore()
    for dev in (z_right, z_left, y_dev, x_right, x_left, mate):
        pl.semaphore_signal(barrier, inc=1, device_id=dev, device_id_type=MESH)
    pl.semaphore_wait(barrier, 6)

    def rows_of(o):
        return pl.ds(mo(o * K, K), K)

    def gu_at(o, ch):
        return gu.at[rows_of(o), pl.ds(mo(par * 896, 128), 384) if ch == A else pl.ds(384, 512)]

    def dn_at(o, ch):
        return dn.at[pl.ds(mo(par * 432, 16), 208) if ch == A else pl.ds(208, 224), rows_of(o)]

    def qb_at(o, ch):
        return qb.at[rows_of(o), pl.ds(mo(par * 256, 128), 128) if ch == A else pl.ds(128, 128)]

    def ob_at(o, ch):
        return ob.at[pl.ds(mo(par * 80, 16), 48) if ch == A else pl.ds(48, 32), rows_of(o)]

    at = (gu_at, dn_at, qb_at, ob_at)
    R = (n - 1) * K
    whole = (
        (gu.at[0:R, 0:384], gu.at[0:R, 384:896]),
        (dn.at[0:208, 0:R], dn.at[208:432, 0:R]),
        (qb.at[0:R, 0:128], qb.at[0:R, 128:256]),
        (ob.at[0:48, 0:R], ob.at[48:80, 0:R]),
    )

    def steps_of(ch, d):
        return H if (ch == A) == (d == RIGHT) else H - 1

    def origin(d, back):
        return lax.rem(zi + n - back, n) if d == RIGHT else lax.rem(zi + back, n)

    def z_copy(m, ch, d, s, o):
        ref = at[m](o, ch)
        return remote(ref, ref, z_send.at[m, ch], z_recv.at[m, d, ch, s - 1], z_dev[d])

    def tick(t):
        for m in range(4):
            s = t - OFFSETS[m]
            if s < 1 or s > H + 1:
                continue
            for ch, d in ((A, RIGHT), (A, LEFT), (B, RIGHT), (B, LEFT)):
                last = steps_of(ch, d)
                if s - 1 > last:
                    continue
                o = origin(d, s - 1)
                if s > 1:
                    z_copy(m, ch, d, s - 1, o).wait_recv()
                if s <= last:
                    z_copy(m, ch, d, s, o).start()
                if s > 1 and ch == A:
                    ref = at[m](o, A)
                    remote(ref, ref, z_send.at[m, 2], c_recv.at[m], y_dev).start()

    def z_done(m):
        w = whole[m][A]
        remote(w, w, z_send.at[m, 2], c_recv.at[m], y_dev).wait_recv()

    H0, H1 = pl.ds(0, D // 2), pl.ds(D // 2, D // 2)
    every = pl.ds(0, D)

    def ag(ph, i, xx, cc, cols, dev):
        ref = xg.at[ph, pl.ds(mo((cc * 4 + xx) * T, 16), T), cols]
        return remote(ref, ref, ag_send.at[ph, i], ag_recv.at[ph, i], dev)

    def ag_start(ph):
        ag(ph, 0, xi, ci, H0, x_right).start()
        ag(ph, 3, xi, ci, H1, x_left).start()
        ag(ph, 6, xi, ci, every, mate).start()
        ag(ph, 1, xi, ci, H1, x_right).start()
        ag(ph, 4, xi, ci, H0, x_left).start()

    def ag_mid(ph):
        ag(ph, 0, x3, ci, H0, x_right).wait_recv()
        ag(ph, 2, x3, ci, H0, x_right).start()
        ag(ph, 7, x3, ci, H0, mate).start()
        ag(ph, 3, x1, ci, H1, x_left).wait_recv()
        ag(ph, 5, x1, ci, H1, x_left).start()
        ag(ph, 10, x1, ci, H1, mate).start()

    def ag_end(ph):
        ag(ph, 1, x3, ci, H1, x_right).wait_recv()
        ag(ph, 8, x3, ci, H1, mate).start()
        ag(ph, 4, x1, ci, H0, x_left).wait_recv()
        ag(ph, 11, x1, ci, H0, mate).start()
        ag(ph, 2, x2, ci, H0, x_right).wait_recv()
        ag(ph, 9, x2, ci, H0, mate).start()
        ag(ph, 5, x2, ci, H1, x_left).wait_recv()
        ag(ph, 12, x2, ci, H1, mate).start()
        ag(ph, 6, xi, oc, every, mate).wait_recv()
        for i, xx, cols in ((7, x3, H0), (10, x1, H1), (8, x3, H1), (11, x1, H0), (9, x2, H0), (12, x2, H1)):
            ag(ph, i, xx, oc, cols, mate).wait_recv()

    def ag_sent(ph):
        for i in range(13):
            ag(ph, i, xi, ci, every if i == 6 else H0, mate).wait_send()

    W = D // CHUNKS
    V = W // 2

    def rs(ph, k, i, dev):
        if i == 6:
            src, dst = pp.at[ph, :, pl.ds(k * W, W)], rp.at[ph, :, pl.ds(k * W, W)]
        else:
            src, dst = st.at[ph, i, :, pl.ds(k * V, V)], rt.at[ph, i, :, pl.ds(k * V, V)]
        return remote(src, dst, rs_send.at[ph, k, i], rs_recv.at[ph, k, i], dev)

    rs_dev = (x_right, x_right, x_right, x_left, x_left, x_left, mate)
    my_rows = pl.ds(mo(ci * 4 * T, 16), 4 * T)
    mate_rows = pl.ds(mo(oc * 4 * T, 16), 4 * T)

    def rs_a(ph, k, hid, wt):
        def other(j, _):
            cols = pl.ds(mo(k * W + j * 256, 256), 256)
            pp[ph, :, cols] = dot(hid[mate_rows, :], wt[:, cols]).astype(bf16)
            return 0

        lax.fori_loop(0, W // 256, other, 0)
        rs(ph, k, 6, mate).start()

        def mine(j, _):
            cols = pl.ds(mo(k * W + j * 256, 256), 256)
            sm[:, cols] = dot(hid[my_rows, :], wt[:, cols])
            return 0

        lax.fori_loop(0, W // 256, mine, 0)

    def part(ph, xx, c0):
        rows, cols = pl.ds(mo(xx * T, 16), T), pl.ds(c0, V)
        return sm[rows, cols] + rp[ph, rows, cols].astype(f32)

    def rs_b(ph, k):
        rs(ph, k, 6, mate).wait_recv()
        lo, hi, to = k * W, k * W + V, pl.ds(k * V, V)
        for i, xx, c0 in ((0, x2, lo), (3, x2, hi), (1, x1, hi), (4, x3, lo)):
            st[ph, i, :, to] = part(ph, xx, c0).astype(bf16)
            rs(ph, k, i, rs_dev[i]).start()

    def rs_c(ph, k):
        lo, hi, to = k * W, k * W + V, pl.ds(k * V, V)
        for i, xx, c0 in ((0, x1, lo), (3, x3, hi)):
            rs(ph, k, i, rs_dev[i]).wait_recv()
            st[ph, i + 2, :, to] = (part(ph, xx, c0) + rt[ph, i, :, to].astype(f32)).astype(bf16)
            rs(ph, k, i + 2, rs_dev[i + 2]).start()

    def rs_d(ph, k):
        lo, hi, to = k * W, k * W + V, pl.ds(k * V, V)
        for i in (1, 4, 2, 5):
            rs(ph, k, i, rs_dev[i]).wait_recv()
        br[:, pl.ds(lo, V)] = part(ph, xi, lo) + rt[ph, 2, :, to].astype(f32) + rt[ph, 4, :, to].astype(f32)
        br[:, pl.ds(hi, V)] = part(ph, xi, hi) + rt[ph, 1, :, to].astype(f32) + rt[ph, 5, :, to].astype(f32)

    def rs_sent(ph):
        for k in range(CHUNKS):
            for i in range(7):
                rs(ph, k, i, rs_dev[i]).wait_send()

    def scatter(ph, hid, wt, between):
        for k in range(CHUNKS):
            rs_a(ph, k, hid, wt)
        for stage in (rs_b, rs_c, rs_d):
            for k in range(CHUNKS):
                stage(ph, k)
                between()

    own_rows = pl.ds(mo((ci * 4 + xi) * T, 16), T)

    def post_norm(ph, scale):
        z = GAIN * xg[ph, own_rows, :].astype(f32) + scale * br[...]
        z = z - jnp.mean(z, axis=-1, keepdims=True)
        return (z * lax.rsqrt(jnp.mean(z * z, axis=-1, keepdims=True) + EPS)).astype(bf16)

    def expand(ph, j0, j1):
        def one(j, _):
            p = dot(xg[ph], gu[:, pl.ds(mo(j * 256, 256), 256)])
            gate, up = p[:, 0:128], p[:, 128:256]
            hb[:, pl.ds(mo(j * 128, 128), 128)] = (gate / (1.0 + jnp.exp(-gate)) * up).astype(bf16)
            return 0

        lax.fori_loop(j0, j1, one, 0)

    def setup_attention():
        t = lax.broadcasted_iota(jnp.int32, (128, 256), 0)
        l = lax.broadcasted_iota(jnp.int32, (128, 256), 1)
        is_key = jnp.where(l >= 128, 1, 0)
        s = l - 128 * is_key
        before = (s + is_key) <= t
        after = (s - is_key) >= t
        for p in range(9):
            if p < 7:
                same = (t >> p) == (s >> p)
                odd = ((t >> p) & 1) == 1
                take = same & ((odd & before) | (jnp.logical_not(odd) & after))
            else:
                take = before if p == 7 else after
            mm[p * 128 : p * 128 + 128, :] = jnp.where(take, 1.0, 0.0).astype(bf16)
        for ref in (qk, lg, og, vb):
            for b in range(2):
                ref[b * PAD + SEQ : b * PAD + PAD, :] = jnp.zeros((PAD - SEQ, 128), ref.dtype)
        for h in range(2):
            lanes = slice(h * 64, h * 64 + 64)
            wle2[:, lanes] = wle[...].astype(f32)
            bias2[:, lanes] = bias[...]
            extra2[:, lanes] = extra[...]

    def place(t):
        return (t // 4) * PAD + (t % 4) * T

    def project():
        a = xg[1]
        p1 = dot(a, qb[:, 0:256])
        p2 = dot(a, qb[:, 256:384])
        low = dot(a, wls[...]).astype(bf16)
        pre = dot(low, wle2[...].astype(bf16)) + bias2[...]
        decay = (jnp.minimum(pre, 0.0) - jnp.log1p(jnp.exp(-jnp.abs(pre)))) / STEEP
        for t in range(8):
            src = ((t % 2) * 4 + t // 2) * T
            to = pl.ds(place(t), T)
            qk[to, :] = p1[src : src + T, 0:128].astype(bf16).astype(f32)
            vb[to, :] = p1[src : src + T, 128:256].astype(bf16)
            og[to, :] = p2[src : src + T, :].astype(bf16).astype(f32)
            lg[to, :] = decay[src : src + T, :] + extra2[t * T : t * T + T, :]

    def attend():
        lane = lax.broadcasted_iota(jnp.int32, (128, 128), 1)
        row = lax.broadcasted_iota(jnp.int32, (128, 128), 0)
        is_q = lane < 64
        differ = row ^ lane

        def sequence(b, _):
            heads, tails, totals, vals, diag = [], [], [], [], []
            for c in range(3):
                rows = pl.ds(mo(b * PAD + c * 128, 128), 128)
                both = qk[rows, :]
                g = lg[rows, :]
                hi = g.astype(bf16)
                lo = (g - hi.astype(f32)).astype(bf16)
                zero = jnp.zeros_like(hi)
                top = jnp.concatenate([jnp.where(is_q, hi, zero), jnp.where(is_q, lo, zero)], axis=1)
                bot = jnp.concatenate([jnp.where(is_q, zero, hi), jnp.where(is_q, zero, lo)], axis=1)
                e = dot(mm[...], jnp.concatenate([top, bot], axis=0))
                e = e[:, 0:128] + e[:, 128:256]
                w = jnp.exp(e)

                def pair(scaled):
                    q = jnp.where(is_q, scaled, 0.0).astype(bf16)
                    return q, pltpu.roll(scaled, 64, 1).astype(bf16)

                scores = dot_t(*pair(both))
                for p in range(7):
                    scores = jnp.where(differ >= (1 << p), dot_t(*pair(both * w[p * 128 : p * 128 + 128])), scores)
                diag.append(scores)
                heads.append(pair(both * w[896:1024]))
                tails.append((both, w[1024:1152], e[1024:1152]))
                totals.append(jnp.sum(g, axis=0, keepdims=True))
                vals.append(vb[rows, :])
                if c == 2:
                    tail = [pair(tails[i][0] * tails[i][1]) for i in range(2)]
                    far = pair(tails[0][0] * jnp.exp(tails[0][2] + totals[1]))
            s01 = dot_t(tail[0][0], heads[1][1])
            s10 = dot_t(heads[1][0], tail[0][1])
            s12 = dot_t(tail[1][0], heads[2][1])
            s21 = dot_t(heads[2][0], tail[1][1])
            s02 = dot_t(far[0], heads[2][1])
            s20 = dot_t(heads[2][0], far[1])
            grid = ((diag[0], s01, s02), (s10, diag[1], s12), (s20, s21, diag[2]))
            for c in range(3):
                rows = pl.ds(mo(b * PAD + c * 128, 128), 128)
                o = sum(dot(grid[c][i].astype(bf16), vals[i]) for i in range(3))
                o = o * lax.rsqrt(jnp.mean(o * o, axis=-1, keepdims=True) + EPS) * gain[...]
                gate = og[rows, :]
                qk[rows, :] = o * (gate / (1.0 + jnp.exp(-gate)))
            return 0

        lax.fori_loop(0, 2, sequence, 0)
        for t in range(8):
            dst = ((t % 2) * 4 + t // 2) * T
            gt[dst : dst + T, :] = qk[pl.ds(place(t), T), :].astype(bf16)

    for c in locals_:
        c.wait()
    tick(1)
    ag_start(0)
    setup_attention()
    tick(2)
    ag_mid(0)
    tick(3)
    ag_end(0)
    clock = [4]
    last_tick = max(OFFSETS) + H + 1

    def advance(upto):
        while clock[0] <= min(upto, last_tick):
            tick(clock[0])
            clock[0] += 1

    advance(OFFSETS[0] + H + 1)
    z_done(0)
    expand(0, 0, 2)
    advance(clock[0])
    expand(0, 2, 4)
    advance(clock[0])
    expand(0, 4, 5)
    advance(OFFSETS[1] + H + 1)
    z_done(1)
    scatter(0, hb, dn, lambda: advance(clock[0]))
    y = post_norm(0, 0.5)
    xg[1, own_rows, :] = y
    ag_start(1)
    advance(clock[0])
    ag_mid(1)
    advance(last_tick)
    ag_end(1)
    z_done(2)
    project()
    attend()
    z_done(3)
    scatter(1, gt, ob, lambda: None)
    y = post_norm(1, 1.0)
    xg[2, own_rows, :] = y
    ag_start(2)
    ag_mid(2)
    ag_end(2)
    expand(2, 0, 5)
    scatter(2, hb, dn, lambda: None)
    out[...] = post_norm(2, 0.5)

    for m in range(4):
        for ch, i in ((A, A), (B, B), (A, 2)):
            w = whole[m][ch]
            remote(w, w, z_send.at[m, i], c_recv.at[m], y_dev).wait_send()
    for ph in range(3):
        ag_sent(ph)
        rs_sent(ph)


def solution(mesh):
    n = mesh.shape["fs"]
    assert mesh.shape["grp"] % 2 == 0 and n % 2 == 0 and mesh.shape["tp"] == 8

    def per_device(x, wsw, wex, wct, wq, wk, wv, wg, wls, wle, bias, extra, gain, wo):
        T, D = x.shape
        K, F = wsw.shape
        N8 = 8 * T
        half = D // 2
        vmem = pl.BlockSpec(memory_space=pltpu.VMEM)
        anywhere = pl.BlockSpec(memory_space=pl.ANY)
        dma = pltpu.SemaphoreType.DMA
        return pl.pallas_call(
            functools.partial(kernel, n),
            out_shape=jax.ShapeDtypeStruct((T, D), bf16),
            in_specs=[anywhere] * 4 + [vmem] * 2 + [anywhere] * 2 + [vmem] * 5 + [anywhere],
            out_specs=vmem,
            scratch_shapes=[
                pltpu.VMEM((D, 2 * F), bf16),
                pltpu.VMEM((F, D), bf16),
                pltpu.VMEM((D, 384), bf16),
                pltpu.VMEM((128, D), bf16),
                pltpu.VMEM((3, N8, D), bf16),
                pltpu.VMEM((N8, F), bf16),
                pltpu.VMEM((3, N8 // 2, D), bf16),
                pltpu.VMEM((3, N8 // 2, D), bf16),
                pltpu.VMEM((N8 // 2, D), f32),
                pltpu.VMEM((3, 6, T, half), bf16),
                pltpu.VMEM((3, 6, T, half), bf16),
                pltpu.VMEM((T, D), f32),
                pltpu.VMEM((2 * PAD, 128), f32),
                pltpu.VMEM((2 * PAD, 128), bf16),
                pltpu.VMEM((2 * PAD, 128), f32),
                pltpu.VMEM((2 * PAD, 128), f32),
                pltpu.VMEM((9 * 128, 256), bf16),
                pltpu.VMEM((wle.shape[0], 128), f32),
                pltpu.VMEM((1, 128), f32),
                pltpu.VMEM((N8, 128), f32),
                pltpu.VMEM((N8, 128), bf16),
                dma((4, 2, 2, n // 2)),
                dma((4,)),
                dma((4, 3)),
                dma((3, 13)),
                dma((3, 13)),
                dma((3, CHUNKS, 7)),
                dma((3, CHUNKS, 7)),
                dma((2 * F // 128 + 5,)),
            ],
            compiler_params=pltpu.CompilerParams(
                collective_id=0, has_side_effects=True, vmem_limit_bytes=60 * 1024 * 1024
            ),
        )(x, wsw, wex, wct, wq, wk, wv, wg, wls, wle, bias.reshape(1, -1), extra, gain.reshape(1, -1), wo)

    return jax.shard_map(
        per_device,
        mesh=mesh,
        in_specs=(
            P(("grp", "fs", "tp"), None),
            P("fs", "tp"),
            P("fs", "tp"),
            P("tp", "fs"),
            P("fs", "tp"),
            P("fs", "tp"),
            P("fs", "tp"),
            P("fs", "tp"),
            P(),
            P(None, "tp"),
            P("tp"),
            P(("grp", "fs"), "tp"),
            P(),
            P("tp", "fs"),
        ),
        out_specs=P(("grp", "fs", "tp"), None),
        check_vma=False,
    )
```

```python
import functools

import jax
import jax.numpy as jnp
from jax import lax
from jax.experimental import pallas as pl
from jax.experimental.pallas import tpu as pltpu
from jax.sharding import PartitionSpec as P

MESH = pl.DeviceIdType.MESH
DK = 64
DV = 128
SEQ = 320
PAD = 384
GAIN = 1.681792830507429
STEEP = 16.0
EPS = 1e-06
CHUNKS = 4
OFFSETS = (0, 3, 9, 0)
NEAR = 5
FIRST = (
    "e0 g0 t0", "e1 g1 t0", "w0 o0 m0", "w1 o1 m1 t0", "b0 w2 o2 m2", "b1 w3 o3 m3", "g2 b2 t0",
    "b3 c0 c1 t0", "c2 c3 t0", "d0 d1 d2 d3",
)
STEPS = ("o0 o1 m0 b0", "o2 m1 b1 o3", "m2 b2 m3 c0", "b3 c1 c2 c3", "d0 d1 d2 d3")
RIGHT, LEFT = 0, 1
A, B = 0, 1
f32, bf16 = jnp.float32, jnp.bfloat16


def mo(v, m):
    return pl.multiple_of(v, m)


def dot(a, b):
    return jnp.dot(a, b, preferred_element_type=f32)


def dot_t(a, b):
    return lax.dot_general(a, b, (((1,), (1,)), ((), ())), preferred_element_type=f32)


def kernel(
    n,
    x_in, wsw, wex, wct, wq_t, wk_t, wv, wg, wls_t, wle_in, bias_in, extra_t, gain_in, wo,
    out,
    gu, dn, qb, wof, ga, xg, hb, pp, rp, sm, st, rt, br,
    qk, vb, og, lg, mm, wle2, bias2, extra2, gt,
    wqk, wls, wle, bias, extra, gain,
    z_recv, c_recv, c_dn, c_ob, z_send, ag_recv, ag_send, rs_recv, rs_send, aa_recv, aa_send, loc,
):
    T, D = x_in.shape
    K = wsw.shape[0]
    F = wsw.shape[1]
    H = n // 2
    zi = lax.axis_index("fs")
    gi = lax.axis_index("grp")
    ti = lax.axis_index("tp")
    par = lax.rem(gi, 2)
    ci = lax.rem(ti, 2)
    xi = lax.div(ti, 2)
    oc = 1 - ci
    x1 = lax.rem(xi + 1, 4)
    x2 = lax.rem(xi + 2, 4)
    x3 = lax.rem(xi + 3, 4)
    z_right = {"fs": lax.rem(zi + 1, n)}
    z_left = {"fs": lax.rem(zi + n - 1, n)}
    y_dev = {"grp": gi + 1 - 2 * par}
    x_right = {"tp": x1 * 2 + ci}
    x_left = {"tp": x3 * 2 + ci}
    mate = {"tp": xi * 2 + oc}
    z_dev = (z_right, z_left)

    def remote(src, dst, s, r, dev):
        return pltpu.make_async_remote_copy(
            src_ref=src, dst_ref=dst, send_sem=s, recv_sem=r, device_id=dev, device_id_type=MESH
        )

    barrier = pltpu.get_barrier_semaphore()
    others = [{"tp": xx * 2 + cc} for xx in (x1, x2, x3) for cc in (ci, oc)]
    for dev in (z_right, z_left, y_dev, mate, *others):
        pl.semaphore_signal(barrier, inc=1, device_id=dev, device_id_type=MESH)

    locals_ = []
    own = pl.ds(mo(zi * K, K), K)
    for j in range(F // 128):
        col = slice(j * 128, j * 128 + 128)
        locals_.append((wsw.at[:, col], gu.at[own, pl.ds(j * 256, 128)]))
        locals_.append((wex.at[:, col], gu.at[own, pl.ds(j * 256 + 128, 128)]))
    locals_.append((x_in, xg.at[0, pl.ds(mo((ci * 4 + xi) * T, 16), T)]))
    locals_.append((wo, wof.at[pl.ds(mo(ti * 128, 128), 128), pl.ds(NEAR * K, K)]))
    first = len(locals_)
    locals_.append((wct, dn.at[:, own]))
    locals_.append((wv, qb.at[own, pl.ds(128, 128)]))
    locals_.append((wg, qb.at[own, pl.ds(256, 128)]))
    locals_.append((wq_t, wqk.at[0]))
    locals_.append((wk_t, wqk.at[1]))
    locals_ += [(wls_t, wls), (wle_in, wle), (bias_in, bias), (extra_t, extra), (gain_in, gain)]
    locals_ = [pltpu.make_async_copy(src, dst, loc.at[i]) for i, (src, dst) in enumerate(locals_)]
    for c in locals_:
        c.start()
    for c in locals_[:first]:
        c.wait()
    pl.semaphore_wait(barrier, 10)

    def rows_of(o):
        return pl.ds(mo(o * K, K), K)

    def gu_at(o, ch):
        return gu.at[rows_of(o), pl.ds(mo(par * 896, 128), 384) if ch == A else pl.ds(384, 512)]

    def dn_at(o, ch):
        return dn.at[pl.ds(mo(par * 432, 16), 208) if ch == A else pl.ds(208, 224), rows_of(o)]

    def qb_at(o, ch):
        return qb.at[rows_of(o), pl.ds(mo(par * 256, 128), 128) if ch == A else pl.ds(128, 128)]

    def ob_at(slot, ch):
        rows = mo(ti * 128 + par * 80, 16) if ch == A else mo(ti * 128 + 48, 16)
        return wof.at[pl.ds(rows, 48 if ch == A else 32), pl.ds(slot * K, K)]

    def ob_slot(d, dist):
        return (NEAR - dist) % n if d == RIGHT else (NEAR + dist) % n

    at = (gu_at, dn_at, qb_at, ob_at)
    R = (n - 1) * K
    whole = (
        (gu.at[0:R, 0:384], gu.at[0:R, 384:896]),
        (dn.at[0:208, 0:R], dn.at[208:432, 0:R]),
        (qb.at[0:R, 0:128], qb.at[0:R, 128:256]),
        (wof.at[0:48, 0:R], wof.at[48:80, 0:R]),
    )

    def steps_of(ch, d):
        return H if (ch == A) == (d == RIGHT) else H - 1

    def origin(d, back):
        return lax.rem(zi + n - back, n) if d == RIGHT else lax.rem(zi + back, n)

    def z_copy(m, ch, d, s, o):
        if m == 3:
            src, dst = ob_at(ob_slot(d, s - 1), ch), ob_at(ob_slot(d, s), ch)
        else:
            src = dst = at[m](o, ch)
        return remote(src, dst, z_send.at[m, ch], z_recv.at[m, d, ch, s - 1], z_dev[d])

    def tick(t):
        for m in range(4):
            s = t - OFFSETS[m]
            if s < 1 or s > H + 1:
                continue
            for ch, d in ((A, RIGHT), (A, LEFT), (B, RIGHT), (B, LEFT)):
                last = steps_of(ch, d)
                if s - 1 > last:
                    continue
                o = origin(d, s - 1)
                if s > 1:
                    z_copy(m, ch, d, s - 1, o).wait_recv()
                if s <= last:
                    z_copy(m, ch, d, s, o).start()
                if s > 1 and ch == A:
                    ref = ob_at(ob_slot(d, s - 1), A) if m == 3 else at[m](o, A)
                    landed = c_recv.at[m]
                    if m == 1:
                        landed = c_dn.at[s - 2, d]
                    elif m == 3:
                        landed = c_ob.at[0 if s - 1 <= NEAR else 1]
                    remote(ref, ref, z_send.at[m, 2], landed, y_dev).start()

    def z_done(m):
        w = whole[m][A]
        remote(w, w, z_send.at[m, 2], c_recv.at[m], y_dev).wait_recv()

    def dn_done(dist, d):
        ref = dn_at(zi, A)
        remote(ref, ref, z_send.at[1, 2], c_dn.at[dist - 1, d], y_dev).wait_recv()

    def ob_done(batch):
        ref = wof.at[0:48, 0 : (2 * NEAR if batch == 0 else n - 1 - 2 * NEAR) * K]
        remote(ref, ref, z_send.at[3, 2], c_ob.at[batch], y_dev).wait_recv()

    def z_sent(m):
        for ch, i in ((A, A), (B, B), (A, 2)):
            w = whole[m][ch]
            remote(w, w, z_send.at[m, i], c_recv.at[m], y_dev).wait_send()

    H0, H1 = pl.ds(0, D // 2), pl.ds(D // 2, D // 2)
    every = pl.ds(0, D)

    near_cols = (2 * NEAR + 1) * K
    batches = ((0, 6 * K, near_cols), (near_cols, near_cols + 3 * K, D))

    def ag(ph, i, xx, cc, cols, dev):
        if ph < 3:
            ref = xg.at[ph, pl.ds(mo((cc * 4 + xx) * T, 16), T), cols]
        else:
            lo, mid, hi = batches[ph - 3]
            cols = pl.ds(lo, mid - lo) if cols is H0 else pl.ds(mid, hi - mid) if cols is H1 else pl.ds(lo, hi - lo)
            ref = wof.at[pl.ds(mo((xx * 2 + cc) * 128, 128), 128), cols]
        return remote(ref, ref, ag_send.at[ph], ag_recv.at[ph, i], dev)

    def ag_start(ph):
        ag(ph, 0, xi, ci, H0, x_right).start()
        ag(ph, 3, xi, ci, H1, x_left).start()
        ag(ph, 6, xi, ci, every, mate).start()
        ag(ph, 1, xi, ci, H1, x_right).start()
        ag(ph, 4, xi, ci, H0, x_left).start()

    def ag_mid(ph):
        ag(ph, 0, x3, ci, H0, x_right).wait_recv()
        ag(ph, 2, x3, ci, H0, x_right).start()
        ag(ph, 7, x3, ci, H0, mate).start()
        ag(ph, 3, x1, ci, H1, x_left).wait_recv()
        ag(ph, 5, x1, ci, H1, x_left).start()
        ag(ph, 10, x1, ci, H1, mate).start()

    def ag_near(ph):
        ag(ph, 1, x3, ci, H1, x_right).wait_recv()
        ag(ph, 8, x3, ci, H1, mate).start()
        ag(ph, 4, x1, ci, H0, x_left).wait_recv()
        ag(ph, 11, x1, ci, H0, mate).start()
        ag(ph, 6, xi, oc, every, mate).wait_recv()
        for i, xx, cols in ((7, x3, H0), (10, x1, H1), (8, x3, H1), (11, x1, H0)):
            ag(ph, i, xx, oc, cols, mate).wait_recv()

    def ag_far(ph):
        ag(ph, 2, x2, ci, H0, x_right).wait_recv()
        ag(ph, 9, x2, ci, H0, mate).start()
        ag(ph, 5, x2, ci, H1, x_left).wait_recv()
        ag(ph, 12, x2, ci, H1, mate).start()

    def ag_end(ph):
        ag(ph, 9, x2, oc, H0, mate).wait_recv()
        ag(ph, 12, x2, oc, H1, mate).wait_recv()

    def ag_sent(ph):
        ref = xg.at[ph, 0 : 7 * T] if ph < 3 else wof.at[0 : 7 * 128, batches[ph - 3][0] : batches[ph - 3][2]]
        remote(ref, ref, ag_send.at[ph], ag_recv.at[ph, 0], mate).wait_send()

    W = D // CHUNKS
    V = W // 2

    def rs(ph, k, i, dev):
        if i == 6:
            src, dst = pp.at[ph, :, pl.ds(k * W, W)], rp.at[ph, :, pl.ds(k * W, W)]
        else:
            src, dst = st.at[ph, i, :, pl.ds(k * V, V)], rt.at[ph, i, :, pl.ds(k * V, V)]
        return remote(src, dst, rs_send.at[ph, i // 6], rs_recv.at[ph, k, i], dev)

    rs_dev = (x_right, x_right, x_right, x_left, x_left, x_left, mate)
    my_rows = pl.ds(mo(ci * 4 * T, 16), 4 * T)
    mate_rows = pl.ds(mo(oc * 4 * T, 16), 4 * T)

    order = [(0, RIGHT)] + [(j // 2 + 1, j % 2) for j in range(n - 1)]
    BLOCKS = W // K

    def columns(ph, slot):
        if ph == 0:
            dist, d = order[slot]
            return pl.ds(mo(origin(d, dist) * K, K), K)
        return pl.ds(slot * K, K)

    def two_blocks(ph, wt, slot):
        if ph == 0:
            return jnp.concatenate([wt[:, columns(ph, slot)], wt[:, columns(ph, slot + 1)]], axis=1)
        return wt[:, pl.ds(slot * K, 2 * K)]

    def rs_o(ph, k, hid, wt):
        for slot in range(k * BLOCKS, (k + 1) * BLOCKS, 2):
            pp[ph, :, pl.ds(slot * K, 2 * K)] = dot(hid[mate_rows, :], two_blocks(ph, wt, slot)).astype(bf16)
        rs(ph, k, 6, mate).start()

    def rs_m(ph, k, hid, wt):
        for slot in range(k * BLOCKS, (k + 1) * BLOCKS, 2):
            sm[:, pl.ds(slot * K, 2 * K)] = dot(hid[my_rows, :], two_blocks(ph, wt, slot))

    def part(ph, xx, c0):
        rows, cols = pl.ds(mo(xx * T, 16), T), pl.ds(c0, V)
        return sm[rows, cols] + rp[ph, rows, cols].astype(f32)

    def rs_b(ph, k):
        rs(ph, k, 6, mate).wait_recv()
        lo, hi, to = k * W, k * W + V, pl.ds(k * V, V)
        for i, xx, c0 in ((0, x2, lo), (3, x2, hi), (1, x1, hi), (4, x3, lo)):
            st[ph, i, :, to] = part(ph, xx, c0).astype(bf16)
            rs(ph, k, i, rs_dev[i]).start()

    def rs_c(ph, k):
        lo, hi, to = k * W, k * W + V, pl.ds(k * V, V)
        for i, xx, c0 in ((0, x1, lo), (3, x3, hi)):
            rs(ph, k, i, rs_dev[i]).wait_recv()
            st[ph, i + 2, :, to] = (part(ph, xx, c0) + rt[ph, i, :, to].astype(f32)).astype(bf16)
            rs(ph, k, i + 2, rs_dev[i + 2]).start()

    def rs_d(ph, k):
        lo, hi, to = k * W, k * W + V, pl.ds(k * V, V)
        for i in (1, 4, 2, 5):
            rs(ph, k, i, rs_dev[i]).wait_recv()
        low = part(ph, xi, lo) + rt[ph, 2, :, to].astype(f32) + rt[ph, 4, :, to].astype(f32)
        high = part(ph, xi, hi) + rt[ph, 1, :, to].astype(f32) + rt[ph, 5, :, to].astype(f32)
        for i in range(BLOCKS // 2):
            br[:, columns(ph, k * BLOCKS + i)] = low[:, i * K : i * K + K]
            br[:, columns(ph, k * BLOCKS + BLOCKS // 2 + i)] = high[:, i * K : i * K + K]

    def rs_sent(ph):
        for i, ref in ((0, st.at[ph]), (1, pp.at[ph])):
            remote(ref, ref, rs_send.at[ph, i], rs_recv.at[ph, 0, 0], mate).wait_send()

    def run(ph, hid, wt, steps, clock=None):
        for step in " ".join(steps).split():
            what, k = step[0], int(step[1:])
            with jax.named_scope(f"rs{ph}_{step}"):
                if what in "wteg":
                    clock(what, k)
                elif what == "o":
                    rs_o(ph, k, hid, wt)
                elif what == "m":
                    rs_m(ph, k, hid, wt)
                else:
                    {"b": rs_b, "c": rs_c, "d": rs_d}[what](ph, k)

    own_rows = pl.ds(mo((ci * 4 + xi) * T, 16), T)

    def post_norm(ph, scale):
        z = GAIN * xg[ph, own_rows, :].astype(f32) + scale * br[...]
        z = z - jnp.mean(z, axis=-1, keepdims=True)
        return (z * lax.rsqrt(jnp.mean(z * z, axis=-1, keepdims=True) + EPS)).astype(bf16)

    def rows_at(cc, xx):
        return pl.ds(mo((cc * 4 + xx) * T, 16), T)

    def expand(ph, j0, j1, chips=None):
        where = None if chips is None else [rows_at(cc, xx) for xx in chips for cc in (0, 1)]

        def one(j, _):
            w = gu[:, pl.ds(mo(j * 256, 256), 256)]
            to = pl.ds(mo(j * 128, 128), 128)
            if where is None:
                p = dot(xg[ph], w)
            else:
                p = dot(jnp.concatenate([xg[ph, r, :] for r in where], axis=0), w)
            gate, up = p[:, 0:128], p[:, 128:256]
            h = (gate / (1.0 + jnp.exp(-gate)) * up).astype(bf16)
            if where is None:
                hb[:, to] = h
            else:
                for i, r in enumerate(where):
                    hb[r, to] = h[i * T : i * T + T, :]
            return 0

        lax.fori_loop(j0, j1, one, 0)

    def setup_attention():
        t = lax.broadcasted_iota(jnp.int32, (128, 256), 0)
        l = lax.broadcasted_iota(jnp.int32, (128, 256), 1)
        is_key = jnp.where(l >= 128, 1, 0)
        s = l - 128 * is_key
        before = (s + is_key) <= t
        after = (s - is_key) >= t
        for p in range(9):
            if p < 7:
                same = (t >> p) == (s >> p)
                odd = ((t >> p) & 1) == 1
                take = same & ((odd & before) | (jnp.logical_not(odd) & after))
            else:
                take = before if p == 7 else after
            mm[p * 128 : p * 128 + 128, :] = jnp.where(take, 1.0, 0.0).astype(bf16)
        for ref in (qk, lg, og, vb):
            for b in range(2):
                ref[b * PAD + SEQ : b * PAD + PAD, :] = jnp.zeros((PAD - SEQ, 128), ref.dtype)
        for h in range(2):
            lanes = slice(h * 64, h * 64 + 64)
            wle2[:, lanes] = wle[...].astype(f32)
            bias2[:, lanes] = bias[...]
            qb[own, lanes] = wqk[h].astype(f32).T.astype(bf16)
            for i in range(8 * T // 128):
                extra2[i * 128 : i * 128 + 128, lanes] = extra[:, i * 128 : i * 128 + 128].T

    def project(b):
        seq = [rows_at(i % 2, 2 * b + i // 2) for i in range(4)]
        a = jnp.concatenate([xg[1, r, :] for r in seq], axis=0)
        to = pl.ds(mo(b * PAD, 128), SEQ)
        p1 = dot(a, qb[:, 0:256])
        qk[to, :] = p1[:, 0:128].astype(bf16).astype(f32)
        vb[to, :] = p1[:, 128:256].astype(bf16)
        og[to, :] = dot(a, qb[:, 256:384]).astype(bf16).astype(f32)
        low = dot_t(a, wls[...]).astype(bf16)
        pre = dot(low, wle2[...].astype(bf16)) + bias2[...]
        decay = (jnp.minimum(pre, 0.0) - jnp.log1p(jnp.exp(-jnp.abs(pre)))) / STEEP
        lg[to, :] = decay + extra2[pl.ds(mo(b * SEQ, 16), SEQ), :]

    def attend(b):
        lane = lax.broadcasted_iota(jnp.int32, (128, 128), 1)
        row = lax.broadcasted_iota(jnp.int32, (128, 128), 0)
        is_q = lane < 64
        differ = row ^ lane

        def sequence():
            heads, tails, totals, vals, diag = [], [], [], [], []
            for c in range(3):
                rows = pl.ds(mo(b * PAD + c * 128, 128), 128)
                both = qk[rows, :]
                g = lg[rows, :]
                hi = g.astype(bf16)
                lo = (g - hi.astype(f32)).astype(bf16)
                zero = jnp.zeros_like(hi)
                top = jnp.concatenate([jnp.where(is_q, hi, zero), jnp.where(is_q, lo, zero)], axis=1)
                bot = jnp.concatenate([jnp.where(is_q, zero, hi), jnp.where(is_q, zero, lo)], axis=1)
                e = dot(mm[...], jnp.concatenate([top, bot], axis=0))
                e = e[:, 0:128] + e[:, 128:256]
                w = jnp.exp(e)

                def pair(scaled):
                    q = jnp.where(is_q, scaled, 0.0).astype(bf16)
                    return q, pltpu.roll(scaled, 64, 1).astype(bf16)

                scores = dot_t(*pair(both))
                for p in range(7):
                    scores = jnp.where(differ >= (1 << p), dot_t(*pair(both * w[p * 128 : p * 128 + 128])), scores)
                diag.append(scores)
                heads.append(pair(both * w[896:1024]))
                tails.append((both, w[1024:1152], e[1024:1152]))
                totals.append(jnp.sum(g, axis=0, keepdims=True))
                vals.append(vb[rows, :])
                if c == 2:
                    tail = [pair(tails[i][0] * tails[i][1]) for i in range(2)]
                    far = pair(tails[0][0] * jnp.exp(tails[0][2] + totals[1]))
            s01 = dot_t(tail[0][0], heads[1][1])
            s10 = dot_t(heads[1][0], tail[0][1])
            s12 = dot_t(tail[1][0], heads[2][1])
            s21 = dot_t(heads[2][0], tail[1][1])
            s02 = dot_t(far[0], heads[2][1])
            s20 = dot_t(heads[2][0], far[1])
            grid = ((diag[0], s01, s02), (s10, diag[1], s12), (s20, s21, diag[2]))
            for c in range(3):
                rows = pl.ds(mo(b * PAD + c * 128, 128), 128)
                o = sum(dot(grid[c][i].astype(bf16), vals[i]) for i in range(3))
                o = o * lax.rsqrt(jnp.mean(o * o, axis=-1, keepdims=True) + EPS) * gain[...]
                gate = og[rows, :]
                qk[rows, :] = o * (gate / (1.0 + jnp.exp(-gate)))

        sequence()
        for i in range(4):
            gt[rows_at(i % 2, 2 * b + i // 2), :] = qk[pl.ds(mo(b * PAD + i * T, 16), T), :].astype(bf16)

    my_cols = pl.ds(mo(ti * 128, 128), 128)

    def hand_out(i, targets):
        for xx, cc in targets:
            remote(gt.at[rows_at(cc, xx)], ga.at[:, my_cols], aa_send.at[i], aa_recv.at[i], {"tp": xx * 2 + cc}).start()

    def handed(i, count):
        ref = gt.at[0 : count * T]
        return remote(ref, ref, aa_send.at[i], aa_recv.at[i], mate)

    def emit():
        for slot in range(0, n, 2):
            p = dot(ga[...], wof[:, slot * K : slot * K + 2 * K])
            for i in range(2):
                o = lax.rem(zi + n + slot + i - NEAR, n)
                br[:, rows_of(o)] = p[:, i * K : i * K + K]

    at_tick = [1]
    last_tick = max(OFFSETS) + H + 1
    scope = jax.named_scope

    def advance(upto):
        while at_tick[0] <= min(upto, last_tick):
            with scope(f"tick_{at_tick[0]}"):
                tick(at_tick[0])
            at_tick[0] += 1

    def landed(k):
        advance(OFFSETS[1] + 2 * k + 3)
        with scope("dn_done"):
            for dist, d in order[max(1, 4 * k) : 4 * k + 4]:
                dn_done(dist, d)

    def more(count):
        advance(at_tick[0] + count - 1)

    advance(1)
    ag_start(0)
    for c in locals_[first:]:
        c.wait()
    with scope("setup"):
        setup_attention()
    advance(2)
    with scope("ag0_mid"):
        ag_mid(0)
    advance(3)
    with scope("ag0_near"):
        ag_near(0)
    with scope("ag0_far"):
        ag_far(0)
    advance(4)
    ag_end(0)
    advance(NEAR + 2)
    with scope("ob_near"):
        ob_done(0)
        ag_start(3)
    advance(NEAR + 3)
    with scope("ob_mid"):
        ag_mid(3)
    advance(OFFSETS[0] + H + 1)
    with scope("ob_far"):
        ag_near(3)
        ag_far(3)
    with scope("gu_done"):
        z_done(0)

    def other(what, k):
        if what == "w":
            landed(k)
        elif what == "t":
            more(1)
        elif what == "g":
            if k == 0:
                ob_done(1)
                ag_start(4)
            elif k == 1:
                ag_mid(4)
            else:
                ag_near(4)
                ag_far(4)
        else:
            expand(0, 3 * k, 3 + 2 * k)

    run(0, hb, dn, FIRST, other)
    with scope("norm"):
        xg[1, own_rows, :] = post_norm(0, 0.5)
    ag_start(1)
    z_sent(0)
    z_sent(1)
    ag_sent(0)
    more(1)
    with scope("ag1_mid"):
        ag_mid(1)
    advance(last_tick)
    with scope("ag1_near"):
        ag_near(1)
    with scope("qb_done"):
        z_done(2)
    seq = lax.div(xi, 2)
    pair = xi + 1 - 2 * lax.rem(xi, 2)
    away = 2 * (1 - seq)
    with scope("project"):
        project(seq)
    with scope("ag1_far"):
        ag_far(1)
    with scope("attend"):
        attend(seq)
        hand_out(0, ((pair, ci), (pair, oc), (xi, oc)))
    with scope("ag1_end"):
        ag_end(1)
    with scope("project"):
        project(1 - seq)
    with scope("attend"):
        attend(1 - seq)
        hand_out(1, ((away, 0), (away, 1), (away + 1, 0), (away + 1, 1)))
    ga[:, my_cols] = gt[own_rows, :]
    with scope("ob_end"):
        ag_end(3)
        ag_end(4)
    with scope("handed"):
        handed(0, 3).wait_recv()
        handed(1, 4).wait_recv()
    with scope("emit"):
        emit()
    with scope("norm"):
        xg[2, own_rows, :] = post_norm(1, 1.0)
    ag_start(2)
    z_sent(2)
    z_sent(3)
    rs_sent(0)
    for i in (1, 3, 4):
        ag_sent(i)
    handed(0, 3).wait_send()
    handed(1, 4).wait_send()
    with scope("ag2_mid"):
        ag_mid(2)
    with scope("ag2_near"):
        ag_near(2)
    near = (xi, x1, x3)
    with scope("expand_near"):
        expand(2, 0, 3, near)
    with scope("ag2_far"):
        ag_far(2)
    with scope("expand_near"):
        expand(2, 3, 5, near)
    with scope("ag2_end"):
        ag_end(2)
    with scope("expand_far"):
        expand(2, 0, 5, (x2,))
    run(1, hb, dn, STEPS)
    with scope("norm"):
        out[...] = post_norm(2, 0.5)
    with scope("sent"):
        ag_sent(2)
        rs_sent(1)


def solution(mesh):
    n = mesh.shape["fs"]
    assert mesh.shape["grp"] % 2 == 0 and n % 2 == 0 and mesh.shape["tp"] == 8

    def per_device(x, wsw, wex, wct, wq, wk, wv, wg, wls, wle, bias, extra, gain, wo):
        T, D = x.shape
        K, F = wsw.shape
        N8 = 8 * T
        half = D // 2
        vmem = pl.BlockSpec(memory_space=pltpu.VMEM)
        anywhere = pl.BlockSpec(memory_space=pl.ANY)
        dma = pltpu.SemaphoreType.DMA
        return pl.pallas_call(
            functools.partial(kernel, n),
            out_shape=jax.ShapeDtypeStruct((T, D), bf16),
            in_specs=[anywhere] * 14,
            out_specs=vmem,
            scratch_shapes=[
                pltpu.VMEM((D, 2 * F), bf16),
                pltpu.VMEM((F, D), bf16),
                pltpu.VMEM((D, 384), bf16),
                pltpu.VMEM((8 * 128, D), bf16),
                pltpu.VMEM((T, 8 * 128), bf16),
                pltpu.VMEM((3, N8, D), bf16),
                pltpu.VMEM((N8, F), bf16),
                pltpu.VMEM((2, N8 // 2, D), bf16),
                pltpu.VMEM((2, N8 // 2, D), bf16),
                pltpu.VMEM((N8 // 2, D), f32),
                pltpu.VMEM((2, 6, T, half), bf16),
                pltpu.VMEM((2, 6, T, half), bf16),
                pltpu.VMEM((T, D), f32),
                pltpu.VMEM((2 * PAD, 128), f32),
                pltpu.VMEM((2 * PAD, 128), bf16),
                pltpu.VMEM((2 * PAD, 128), f32),
                pltpu.VMEM((2 * PAD, 128), f32),
                pltpu.VMEM((9 * 128, 256), bf16),
                pltpu.VMEM((wle.shape[0], 128), f32),
                pltpu.VMEM((1, 128), f32),
                pltpu.VMEM((N8, 128), f32),
                pltpu.VMEM((N8, 128), bf16),
                pltpu.VMEM((2, wq.shape[1], K), bf16),
                pltpu.VMEM((wls.shape[1], D), bf16),
                pltpu.VMEM(wle.shape, bf16),
                pltpu.VMEM((1, bias.shape[0]), f32),
                pltpu.VMEM((extra.shape[1], extra.shape[0]), f32),
                pltpu.VMEM((1, gain.shape[0]), f32),
                dma((4, 2, 2, n // 2)),
                dma((4,)),
                dma((n // 2, 2)),
                dma((2,)),
                dma((4, 3)),
                dma((5, 13)),
                dma((5,)),
                dma((2, CHUNKS, 7)),
                dma((2, 2)),
                dma((2,)),
                dma((2,)),
                dma((2 * F // 128 + 12,)),
            ],
            compiler_params=pltpu.CompilerParams(
                collective_id=0, has_side_effects=True, vmem_limit_bytes=60 * 1024 * 1024
            ),
        )(
            x, wsw, wex, wct, wq.T, wk.T, wv, wg, wls.T, wle, bias.reshape(1, -1), extra.T, gain.reshape(1, -1), wo
        )

    return jax.shard_map(
        per_device,
        mesh=mesh,
        in_specs=(
            P(("grp", "fs", "tp"), None),
            P("fs", "tp"),
            P("fs", "tp"),
            P("tp", "fs"),
            P("fs", "tp"),
            P("fs", "tp"),
            P("fs", "tp"),
            P("fs", "tp"),
            P(),
            P(None, "tp"),
            P("tp"),
            P(("grp", "fs"), "tp"),
            P(),
            P("tp", "fs"),
        ),
        out_specs=P(("grp", "fs", "tp"), None),
        check_vma=False,
    )
```

```python
import functools

import jax
import jax.numpy as jnp
from jax import lax
from jax.experimental import pallas as pl
from jax.experimental.pallas import tpu as pltpu
from jax.sharding import PartitionSpec as P

MESH = pl.DeviceIdType.MESH
DK = 64
DV = 128
SEQ = 320
PAD = 384
GAIN = 1.681792830507429
STEEP = 16.0
EPS = 1e-06
CHUNKS = 4
OFFSETS = (0, 3, 9, 0)
NEAR = 5
FIRST = (
    "t0 w0 o0 m0", "w1 o1 m1 t0", "b0 b1 w2 o2", "m2 t0 b2 c0", "c1 w3 o3 m3", "b3 c2 t0 g2",
    "c3 d0 d1 t0", "d2 d3",
)
STEPS = ("o0 o1 m0 b0", "o2 m1 b1 o3", "m2 b2 m3 c0", "b3 c1 c2 c3", "d0 d1 d2 d3")
RIGHT, LEFT = 0, 1
A, B = 0, 1
f32, bf16 = jnp.float32, jnp.bfloat16


def mo(v, m):
    return pl.multiple_of(v, m)


def dot(a, b):
    return jnp.dot(a, b, preferred_element_type=f32)


def dot_t(a, b):
    return lax.dot_general(a, b, (((1,), (1,)), ((), ())), preferred_element_type=f32)


def kernel(
    n,
    x_in, wsw, wex, wct, wq_t, wk_t, wv, wg, wls_t, wle_in, bias_in, extra_t, gain_in, wo,
    out,
    gu, dn, qb, wof, ga, xg, acc, hb, pp, rp, sm, st, rt, br,
    qk, vb, og, lg, mm, wle2, bias2, extra2, gt,
    wqk, wls, wle, bias, extra, gain,
    z_recv, c_gu, c_dn, c_qb, c_ob, z_send, ag_recv, ag_send, rs_recv, rs_send, aa_recv, aa_send, loc,
):
    T, D = x_in.shape
    K = wsw.shape[0]
    F = wsw.shape[1]
    H = n // 2
    zi = lax.axis_index("fs")
    gi = lax.axis_index("grp")
    ti = lax.axis_index("tp")
    par = lax.rem(gi, 2)
    ci = lax.rem(ti, 2)
    xi = lax.div(ti, 2)
    oc = 1 - ci
    x1 = lax.rem(xi + 1, 4)
    x2 = lax.rem(xi + 2, 4)
    x3 = lax.rem(xi + 3, 4)
    z_right = {"fs": lax.rem(zi + 1, n)}
    z_left = {"fs": lax.rem(zi + n - 1, n)}
    y_dev = {"grp": gi + 1 - 2 * par}
    x_right = {"tp": x1 * 2 + ci}
    x_left = {"tp": x3 * 2 + ci}
    mate = {"tp": xi * 2 + oc}
    z_dev = (z_right, z_left)

    def remote(src, dst, s, r, dev):
        return pltpu.make_async_remote_copy(
            src_ref=src, dst_ref=dst, send_sem=s, recv_sem=r, device_id=dev, device_id_type=MESH
        )

    barrier = pltpu.get_barrier_semaphore()
    others = [{"tp": xx * 2 + cc} for xx in (x1, x2, x3) for cc in (ci, oc)]
    for dev in (z_right, z_left, y_dev, mate, *others):
        pl.semaphore_signal(barrier, inc=1, device_id=dev, device_id_type=MESH)

    locals_ = []
    own = pl.ds(mo(zi * K, K), K)
    for j in range(F // 128):
        col = slice(j * 128, j * 128 + 128)
        pltpu.make_async_copy(wsw.at[:, col], gu.at[own, pl.ds(j * 256, 128)], loc.at[12]).start()
        pltpu.make_async_copy(wex.at[:, col], gu.at[own, pl.ds(j * 256 + 128, 128)], loc.at[12]).start()
    locals_.append((x_in, xg.at[0, pl.ds(mo((ci * 4 + xi) * T, 16), T)]))
    locals_.append((wo, wof.at[pl.ds(mo(ti * 128, 128), 128), pl.ds(NEAR * K, K)]))
    first = len(locals_)
    locals_.append((wct, dn.at[:, own]))
    locals_.append((wv, qb.at[own, pl.ds(128, 128)]))
    locals_.append((wg, qb.at[own, pl.ds(256, 128)]))
    locals_.append((wq_t, wqk.at[0]))
    locals_.append((wk_t, wqk.at[1]))
    locals_ += [(wls_t, wls), (wle_in, wle), (bias_in, bias), (extra_t, extra), (gain_in, gain)]
    locals_ = [pltpu.make_async_copy(src, dst, loc.at[i]) for i, (src, dst) in enumerate(locals_)]
    for c in locals_:
        c.start()
    for c in locals_[:first]:
        c.wait()
    pltpu.make_async_copy(gu.at[own], gu.at[own], loc.at[12]).wait()
    pl.semaphore_wait(barrier, 10)

    def rows_of(o):
        return pl.ds(mo(o * K, K), K)

    def gu_at(o, ch):
        return gu.at[rows_of(o), pl.ds(mo(par * 896, 128), 384) if ch == A else pl.ds(384, 512)]

    def dn_at(o, ch):
        return dn.at[pl.ds(mo(par * 432, 16), 208) if ch == A else pl.ds(208, 224), rows_of(o)]

    def qb_at(o, ch):
        return qb.at[rows_of(o), pl.ds(mo(par * 256, 128), 128) if ch == A else pl.ds(128, 128)]

    def ob_at(slot, ch):
        rows = mo(ti * 128 + par * 80, 16) if ch == A else mo(ti * 128 + 48, 16)
        return wof.at[pl.ds(rows, 48 if ch == A else 32), pl.ds(slot * K, K)]

    def ob_slot(d, dist):
        return (NEAR - dist) % n if d == RIGHT else (NEAR + dist) % n

    at = (gu_at, dn_at, qb_at, ob_at)
    R = (n - 1) * K
    whole = (
        (gu.at[0:R, 0:384], gu.at[0:R, 384:896]),
        (dn.at[0:208, 0:R], dn.at[208:432, 0:R]),
        (qb.at[0:R, 0:128], qb.at[0:R, 128:256]),
        (wof.at[0:48, 0:R], wof.at[48:80, 0:R]),
    )

    def steps_of(ch, d):
        return H if (ch == A) == (d == RIGHT) else H - 1

    def origin(d, back):
        return lax.rem(zi + n - back, n) if d == RIGHT else lax.rem(zi + back, n)

    def z_copy(m, ch, d, s, o):
        if m == 3:
            src, dst = ob_at(ob_slot(d, s - 1), ch), ob_at(ob_slot(d, s), ch)
        else:
            src = dst = at[m](o, ch)
        return remote(src, dst, z_send.at[m, ch], z_recv.at[(0, 1, 0, 2)[m], d, ch, s - 1], z_dev[d])

    def tick(t):
        for m in range(4):
            s = t - OFFSETS[m]
            if s < 1 or s > H + 1:
                continue
            for ch, d in ((A, RIGHT), (A, LEFT), (B, RIGHT), (B, LEFT)):
                last = steps_of(ch, d)
                if s - 1 > last:
                    continue
                o = origin(d, s - 1)
                if s > 1:
                    z_copy(m, ch, d, s - 1, o).wait_recv()
                if s <= last:
                    z_copy(m, ch, d, s, o).start()
                if s > 1 and ch == A:
                    ref = ob_at(ob_slot(d, s - 1), A) if m == 3 else at[m](o, A)
                    landed = (c_gu.at[s - 2], c_dn.at[s - 2], c_qb.at[0], c_ob.at[0 if s - 1 <= NEAR else 1])[m]
                    remote(ref, ref, z_send.at[m, 2], landed, y_dev).start()

    def qb_done():
        w = whole[2][A]
        remote(w, w, z_send.at[2, 2], c_qb.at[0], y_dev).wait_recv()

    def gu_done(dist):
        ref = gu.at[0 : (2 if dist < H else 1) * K, 0:384]
        remote(ref, ref, z_send.at[0, 2], c_gu.at[dist - 1], y_dev).wait_recv()

    def dn_done(dist):
        ref = dn.at[0:208, 0 : (2 if dist < H else 1) * K]
        remote(ref, ref, z_send.at[1, 2], c_dn.at[dist - 1], y_dev).wait_recv()

    def ob_done(batch):
        ref = wof.at[0:48, 0 : (2 * NEAR if batch == 0 else n - 1 - 2 * NEAR) * K]
        remote(ref, ref, z_send.at[3, 2], c_ob.at[batch], y_dev).wait_recv()

    def z_sent(m):
        for ch, i in ((A, A), (B, B), (A, 2)):
            w = whole[m][ch]
            remote(w, w, z_send.at[m, i], c_qb.at[0], y_dev).wait_send()

    H0, H1 = pl.ds(0, D // 2), pl.ds(D // 2, D // 2)
    every = pl.ds(0, D)

    near_cols = (2 * NEAR + 1) * K
    batches = ((0, 6 * K, near_cols), (near_cols, near_cols + 3 * K, D))

    def ag(ph, i, xx, cc, cols, dev):
        if ph < 3:
            ref = xg.at[ph, pl.ds(mo((cc * 4 + xx) * T, 16), T), cols]
        else:
            lo, mid, hi = batches[ph - 3]
            cols = pl.ds(lo, mid - lo) if cols is H0 else pl.ds(mid, hi - mid) if cols is H1 else pl.ds(lo, hi - lo)
            ref = wof.at[pl.ds(mo((xx * 2 + cc) * 128, 128), 128), cols]
        slot = i if i < 7 else 8 if i in (9, 12) else 7
        return remote(ref, ref, ag_send.at[ph], ag_recv.at[ph, slot], dev)

    def from_mate(ph, slot, count):
        rows = count * (T if ph < 3 else 128)
        ref = xg.at[ph, 0:rows] if ph < 3 else wof.at[0:rows, batches[ph - 3][0] : batches[ph - 3][2]]
        remote(ref, ref, ag_send.at[ph], ag_recv.at[ph, slot], mate).wait_recv()

    def ag_start(ph):
        ag(ph, 0, xi, ci, H0, x_right).start()
        ag(ph, 3, xi, ci, H1, x_left).start()
        ag(ph, 6, xi, ci, every, mate).start()
        ag(ph, 1, xi, ci, H1, x_right).start()
        ag(ph, 4, xi, ci, H0, x_left).start()

    def ag_mid(ph):
        ag(ph, 0, x3, ci, H0, x_right).wait_recv()
        ag(ph, 2, x3, ci, H0, x_right).start()
        ag(ph, 7, x3, ci, H0, mate).start()
        ag(ph, 3, x1, ci, H1, x_left).wait_recv()
        ag(ph, 5, x1, ci, H1, x_left).start()
        ag(ph, 10, x1, ci, H1, mate).start()

    def ag_near(ph):
        ag(ph, 1, x3, ci, H1, x_right).wait_recv()
        ag(ph, 8, x3, ci, H1, mate).start()
        ag(ph, 4, x1, ci, H0, x_left).wait_recv()
        ag(ph, 11, x1, ci, H0, mate).start()
        if ph != 2:
            from_mate(ph, 6, 1)
        from_mate(ph, 7, 2)

    def ag_far(ph):
        ag(ph, 2, x2, ci, H0, x_right).wait_recv()
        ag(ph, 9, x2, ci, H0, mate).start()
        ag(ph, 5, x2, ci, H1, x_left).wait_recv()
        ag(ph, 12, x2, ci, H1, mate).start()

    def ag_end(ph):
        from_mate(ph, 8, 1)

    def ag_sent(ph):
        ref = xg.at[ph, 0 : 7 * T] if ph < 3 else wof.at[0 : 7 * 128, batches[ph - 3][0] : batches[ph - 3][2]]
        remote(ref, ref, ag_send.at[ph], ag_recv.at[ph, 0], mate).wait_send()

    W = D // CHUNKS
    V = W // 2

    def rs(ph, k, i, dev):
        if i == 6:
            src, dst = pp.at[ph, :, pl.ds(k * W, W)], rp.at[ph, :, pl.ds(k * W, W)]
        else:
            src, dst = st.at[ph, i, :, pl.ds(k * V, V)], rt.at[ph, i, :, pl.ds(k * V, V)]
        return remote(src, dst, rs_send.at[ph, i // 6], rs_recv.at[ph, k, (0, 2, 2, 1, 2, 2, 3)[i]], dev)

    rs_dev = (x_right, x_right, x_right, x_left, x_left, x_left, mate)
    my_rows = pl.ds(mo(ci * 4 * T, 16), 4 * T)
    mate_rows = pl.ds(mo(oc * 4 * T, 16), 4 * T)

    order = [(0, RIGHT)] + [(j // 2 + 1, j % 2) for j in range(n - 1)]
    BLOCKS = W // K

    def columns(ph, slot):
        if ph == 0:
            dist, d = order[slot]
            return pl.ds(mo(origin(d, dist) * K, K), K)
        return pl.ds(slot * K, K)

    def two_blocks(ph, wt, slot):
        if ph == 0:
            return jnp.concatenate([wt[:, columns(ph, slot)], wt[:, columns(ph, slot + 1)]], axis=1)
        return wt[:, pl.ds(slot * K, 2 * K)]

    def rs_o(ph, k, hid, wt):
        for slot in range(k * BLOCKS, (k + 1) * BLOCKS, 2):
            pp[ph, :, pl.ds(slot * K, 2 * K)] = dot(hid[mate_rows, :], two_blocks(ph, wt, slot)).astype(bf16)
        rs(ph, k, 6, mate).start()

    def rs_m(ph, k, hid, wt):
        for slot in range(k * BLOCKS, (k + 1) * BLOCKS, 2):
            sm[:, pl.ds(slot * K, 2 * K)] = dot(hid[my_rows, :], two_blocks(ph, wt, slot))

    def part(ph, xx, c0):
        rows, cols = pl.ds(mo(xx * T, 16), T), pl.ds(c0, V)
        return sm[rows, cols] + rp[ph, rows, cols].astype(f32)

    def rs_b(ph, k):
        rs(ph, k, 6, mate).wait_recv()
        lo, hi, to = k * W, k * W + V, pl.ds(k * V, V)
        for i, xx, c0 in ((0, x2, lo), (3, x2, hi), (1, x1, hi), (4, x3, lo)):
            st[ph, i, :, to] = part(ph, xx, c0).astype(bf16)
            rs(ph, k, i, rs_dev[i]).start()

    def rs_c(ph, k):
        lo, hi, to = k * W, k * W + V, pl.ds(k * V, V)
        for i, xx, c0 in ((0, x1, lo), (3, x3, hi)):
            rs(ph, k, i, rs_dev[i]).wait_recv()
            st[ph, i + 2, :, to] = (part(ph, xx, c0) + rt[ph, i, :, to].astype(f32)).astype(bf16)
            rs(ph, k, i + 2, rs_dev[i + 2]).start()

    def rs_d(ph, k):
        lo, hi, to = k * W, k * W + V, pl.ds(k * V, V)
        ref = rt.at[ph, 0:4, :, pl.ds(0, V)]
        remote(ref, ref, rs_send.at[ph, 0], rs_recv.at[ph, k, 2], mate).wait_recv()
        low = part(ph, xi, lo) + rt[ph, 2, :, to].astype(f32) + rt[ph, 4, :, to].astype(f32)
        high = part(ph, xi, hi) + rt[ph, 1, :, to].astype(f32) + rt[ph, 5, :, to].astype(f32)
        for i in range(BLOCKS // 2):
            br[:, columns(ph, k * BLOCKS + i)] = low[:, i * K : i * K + K]
            br[:, columns(ph, k * BLOCKS + BLOCKS // 2 + i)] = high[:, i * K : i * K + K]

    def rs_sent(ph):
        for i, ref in ((0, st.at[ph]), (1, pp.at[ph])):
            remote(ref, ref, rs_send.at[ph, i], rs_recv.at[ph, 0, 0], mate).wait_send()

    def run(ph, hid, wt, steps, clock=None):
        for step in " ".join(steps).split():
            what, k = step[0], int(step[1:])
            with jax.named_scope(f"rs{ph}_{step}"):
                if what in "wteg":
                    clock(what, k)
                elif what == "o":
                    rs_o(ph, k, hid, wt)
                elif what == "m":
                    rs_m(ph, k, hid, wt)
                else:
                    {"b": rs_b, "c": rs_c, "d": rs_d}[what](ph, k)

    own_rows = pl.ds(mo((ci * 4 + xi) * T, 16), T)

    def post_norm(ph, scale):
        z = GAIN * xg[ph, own_rows, :].astype(f32) + scale * br[...]
        z = z - jnp.mean(z, axis=-1, keepdims=True)
        return (z * lax.rsqrt(jnp.mean(z * z, axis=-1, keepdims=True) + EPS)).astype(bf16)

    def rows_at(cc, xx):
        return pl.ds(mo((cc * 4 + xx) * T, 16), T)

    def expand(ph, j0, j1, chips):
        where = [rows_at(cc, xx) for xx in chips for cc in (0, 1)]

        def one(j, _):
            w = gu[:, pl.ds(mo(j * 256, 256), 256)]
            to = pl.ds(mo(j * 128, 128), 128)
            p = dot(jnp.concatenate([xg[ph, r, :] for r in where], axis=0), w)
            gate, up = p[:, 0:128], p[:, 128:256]
            h = (gate / (1.0 + jnp.exp(-gate)) * up).astype(bf16)
            for i, r in enumerate(where):
                hb[r, to] = h[i * T : i * T + T, :]
            return 0

        lax.fori_loop(j0, j1, one, 0)

    def accumulate(o1, o2, first=False, last=False):
        def one(j, _):
            cols = pl.ds(mo(j * 256, 256), 256)
            w = jnp.concatenate([gu[rows_of(o1), cols], gu[rows_of(o2), cols]], axis=0)
            p = dot(jnp.concatenate([xg[0, :, rows_of(o1)], xg[0, :, rows_of(o2)]], axis=1), w)
            if not first:
                p = p + acc[:, cols]
            if last:
                gate, up = p[:, 0:128], p[:, 128:256]
                hb[:, pl.ds(mo(j * 128, 128), 128)] = (gate / (1.0 + jnp.exp(-gate)) * up).astype(bf16)
            else:
                acc[:, cols] = p
            return 0

        lax.fori_loop(0, F // 128, one, 0)

    def expand_pair(dist):
        with jax.named_scope(f"pair_{dist}"):
            gu_done(dist)
            if dist == H:
                accumulate(zi, origin(LEFT, H), last=True)
            else:
                accumulate(origin(RIGHT, dist), origin(LEFT, dist), first=dist == 1)

    def setup_attention():
        t = lax.broadcasted_iota(jnp.int32, (128, 256), 0)
        l = lax.broadcasted_iota(jnp.int32, (128, 256), 1)
        is_key = jnp.where(l >= 128, 1, 0)
        s = l - 128 * is_key
        before = (s + is_key) <= t
        after = (s - is_key) >= t
        for p in range(9):
            if p < 7:
                same = (t >> p) == (s >> p)
                odd = ((t >> p) & 1) == 1
                take = same & ((odd & before) | (jnp.logical_not(odd) & after))
            else:
                take = before if p == 7 else after
            mm[p * 128 : p * 128 + 128, :] = jnp.where(take, 1.0, 0.0).astype(bf16)
        for ref in (qk, lg, og, vb):
            for b in range(2):
                ref[b * PAD + SEQ : b * PAD + PAD, :] = jnp.zeros((PAD - SEQ, 128), ref.dtype)
        for h in range(2):
            lanes = slice(h * 64, h * 64 + 64)
            wle2[:, lanes] = wle[...].astype(f32)
            bias2[:, lanes] = bias[...]
            qb[own, lanes] = wqk[h].astype(f32).T.astype(bf16)
        qb[:, 384:512] = jnp.zeros((D, 128), bf16)
        for i in range(D // 128):
            qb[i * 128 : i * 128 + 128, 384 : 384 + wls.shape[0]] = (
                wls[:, i * 128 : i * 128 + 128].astype(f32).T.astype(bf16)
            )
        for h in range(2):
            lanes = slice(h * 64, h * 64 + 64)
            for i in range(8 * T // 128):
                extra2[i * 128 : i * 128 + 128, lanes] = extra[:, i * 128 : i * 128 + 128].T

    def project(b):
        seq = [rows_at(i % 2, 2 * b + i // 2) for i in range(4)]
        a = jnp.concatenate([xg[1, r, :] for r in seq], axis=0)
        to = pl.ds(mo(b * PAD, 128), SEQ)
        p1 = dot(a, qb[:, 0:256])
        qk[to, :] = p1[:, 0:128].astype(bf16).astype(f32)
        vb[to, :] = p1[:, 128:256].astype(bf16)
        p2 = dot(a, qb[:, 256:512])
        og[to, :] = p2[:, 0:128].astype(bf16).astype(f32)
        low = p2[:, 128 : 128 + wls.shape[0]].astype(bf16)
        pre = dot(low, wle2[...].astype(bf16)) + bias2[...]
        decay = (jnp.minimum(pre, 0.0) - jnp.log1p(jnp.exp(-jnp.abs(pre)))) / STEEP
        lg[to, :] = decay + extra2[pl.ds(mo(b * SEQ, 16), SEQ), :]

    def attend(b):
        lane = lax.broadcasted_iota(jnp.int32, (128, 128), 1)
        row = lax.broadcasted_iota(jnp.int32, (128, 128), 0)
        is_q = lane < 64
        differ = row ^ lane

        def sequence():
            heads, tails, totals, vals, diag = [], [], [], [], []
            for c in range(3):
                rows = pl.ds(mo(b * PAD + c * 128, 128), 128)
                both = qk[rows, :]
                g = lg[rows, :]
                hi = g.astype(bf16)
                lo = (g - hi.astype(f32)).astype(bf16)
                zero = jnp.zeros_like(hi)
                top = jnp.concatenate([jnp.where(is_q, hi, zero), jnp.where(is_q, lo, zero)], axis=1)
                bot = jnp.concatenate([jnp.where(is_q, zero, hi), jnp.where(is_q, zero, lo)], axis=1)
                e = dot(mm[...], jnp.concatenate([top, bot], axis=0))
                e = e[:, 0:128] + e[:, 128:256]
                w = jnp.exp(e)

                def pair(scaled):
                    q = jnp.where(is_q, scaled, 0.0).astype(bf16)
                    return q, pltpu.roll(scaled, 64, 1).astype(bf16)

                scores = dot_t(*pair(both))
                for p in range(7):
                    scores = jnp.where(differ >= (1 << p), dot_t(*pair(both * w[p * 128 : p * 128 + 128])), scores)
                diag.append(scores)
                heads.append(pair(both * w[896:1024]))
                tails.append((both, w[1024:1152], e[1024:1152]))
                totals.append(jnp.sum(g, axis=0, keepdims=True))
                vals.append(vb[rows, :])
                if c == 2:
                    tail = [pair(tails[i][0] * tails[i][1]) for i in range(2)]
                    far = pair(tails[0][0] * jnp.exp(tails[0][2] + totals[1]))
            s01 = dot_t(tail[0][0], heads[1][1])
            s10 = dot_t(heads[1][0], tail[0][1])
            s12 = dot_t(tail[1][0], heads[2][1])
            s21 = dot_t(heads[2][0], tail[1][1])
            s02 = dot_t(far[0], heads[2][1])
            s20 = dot_t(heads[2][0], far[1])
            grid = ((diag[0], s01, s02), (s10, diag[1], s12), (s20, s21, diag[2]))
            for c in range(3):
                rows = pl.ds(mo(b * PAD + c * 128, 128), 128)
                o = sum(dot(grid[c][i].astype(bf16), vals[i]) for i in range(3))
                o = o * lax.rsqrt(jnp.mean(o * o, axis=-1, keepdims=True) + EPS) * gain[...]
                gate = og[rows, :]
                qk[rows, :] = o * (gate / (1.0 + jnp.exp(-gate)))

        sequence()
        for i in range(4):
            gt[rows_at(i % 2, 2 * b + i // 2), :] = qk[pl.ds(mo(b * PAD + i * T, 16), T), :].astype(bf16)

    my_cols = pl.ds(mo(ti * 128, 128), 128)

    def hand_out(i, targets):
        for xx, cc in targets:
            remote(gt.at[rows_at(cc, xx)], ga.at[:, my_cols], aa_send.at[i], aa_recv.at[i], {"tp": xx * 2 + cc}).start()

    def handed(i, count):
        ref = gt.at[0 : count * T]
        return remote(ref, ref, aa_send.at[i], aa_recv.at[i], mate)

    def emit():
        for slot in range(0, n, 2):
            p = dot(ga[...], wof[:, slot * K : slot * K + 2 * K])
            for i in range(2):
                o = lax.rem(zi + n + slot + i - NEAR, n)
                br[:, rows_of(o)] = p[:, i * K : i * K + K]

    at_tick = [1]
    last_tick = max(OFFSETS) + H + 1
    scope = jax.named_scope

    def advance(upto):
        while at_tick[0] <= min(upto, last_tick):
            with scope(f"tick_{at_tick[0]}"):
                tick(at_tick[0])
            at_tick[0] += 1

    def landed(k):
        advance(OFFSETS[1] + 2 * k + 3)
        with scope("dn_done"):
            dn_done(2 * k + 1)
            dn_done(2 * k + 2)

    def more(count):
        advance(at_tick[0] + count - 1)

    advance(1)
    ag_start(0)
    for c in locals_[first:]:
        c.wait()
    with scope("setup"):
        setup_attention()
    advance(2)
    with scope("ag0_mid"):
        ag_mid(0)
    advance(3)
    with scope("ag0_near"):
        ag_near(0)
    with scope("ag0_far"):
        ag_far(0)
    advance(4)
    ag_end(0)
    advance(5)
    for dist in (1, 2, 3):
        expand_pair(dist)
    advance(6)
    expand_pair(4)
    advance(7)
    with scope("ob_near"):
        ob_done(0)
        ag_start(3)
    expand_pair(5)
    advance(8)
    with scope("ob_mid"):
        ag_mid(3)
    expand_pair(6)
    expand_pair(7)
    advance(9)
    expand_pair(8)

    def other(what, k):
        if what == "w":
            landed(k)
        elif what == "t":
            more(1)
        else:
            ag_near(3)
            ag_far(3)

    run(0, hb, dn, FIRST, other)
    with scope("norm"):
        xg[1, own_rows, :] = post_norm(0, 0.5)
    ag_start(1)
    z_sent(0)
    z_sent(1)
    ag_sent(0)
    more(2)
    with scope("ag1_mid"):
        ag_mid(1)
    advance(last_tick)
    with scope("ag1_near"):
        ag_near(1)
    with scope("qb_done"):
        qb_done()
        ob_done(1)
        ag_start(4)
    seq = lax.div(xi, 2)
    pair = xi + 1 - 2 * lax.rem(xi, 2)
    away = 2 * (1 - seq)
    with scope("project"):
        project(seq)
    with scope("ag1_far"):
        ag_far(1)
    with scope("attend"):
        attend(seq)
        hand_out(0, ((pair, ci), (pair, oc), (xi, oc)))
    with scope("ag1_end"):
        ag_end(1)
    with scope("project"):
        project(1 - seq)
    with scope("ob2_mid"):
        ag_mid(4)
    with scope("attend"):
        attend(1 - seq)
        hand_out(1, ((away, 0), (away, 1), (away + 1, 0), (away + 1, 1)))
    ga[:, my_cols] = gt[own_rows, :]
    with scope("ob2_far"):
        ag_near(4)
        ag_far(4)
    with scope("ob_end"):
        ag_end(3)
        ag_end(4)
    with scope("handed"):
        handed(0, 3).wait_recv()
        handed(1, 4).wait_recv()
    with scope("emit"):
        emit()
    with scope("norm"):
        xg[2, own_rows, :] = post_norm(1, 1.0)
    ag_start(2)
    z_sent(2)
    z_sent(3)
    rs_sent(0)
    for i in (1, 3, 4):
        ag_sent(i)
    handed(0, 3).wait_send()
    handed(1, 4).wait_send()
    with scope("expand_own"):
        from_mate(2, 6, 1)
        expand(2, 0, 5, (xi,))
    with scope("ag2_mid"):
        ag_mid(2)
    with scope("ag2_near"):
        ag_near(2)
    near = (x1, x3)
    with scope("expand_near"):
        expand(2, 0, 3, near)
    with scope("ag2_far"):
        ag_far(2)
    with scope("expand_near"):
        expand(2, 3, 5, near)
    with scope("ag2_end"):
        ag_end(2)
    with scope("expand_far"):
        expand(2, 0, 5, (x2,))
    run(1, hb, dn, STEPS)
    with scope("norm"):
        out[...] = post_norm(2, 0.5)
    with scope("sent"):
        ag_sent(2)
        rs_sent(1)


def solution(mesh):
    n = mesh.shape["fs"]
    assert mesh.shape["grp"] % 2 == 0 and n % 2 == 0 and mesh.shape["tp"] == 8

    def per_device(x, wsw, wex, wct, wq, wk, wv, wg, wls, wle, bias, extra, gain, wo):
        T, D = x.shape
        K, F = wsw.shape
        N8 = 8 * T
        half = D // 2
        vmem = pl.BlockSpec(memory_space=pltpu.VMEM)
        anywhere = pl.BlockSpec(memory_space=pl.ANY)
        dma = pltpu.SemaphoreType.DMA
        return pl.pallas_call(
            functools.partial(kernel, n),
            out_shape=jax.ShapeDtypeStruct((T, D), bf16),
            in_specs=[anywhere] * 14,
            out_specs=vmem,
            scratch_shapes=[
                pltpu.VMEM((D, 2 * F), bf16),
                pltpu.VMEM((F, D), bf16),
                pltpu.VMEM((D, 512), bf16),
                pltpu.VMEM((8 * 128, D), bf16),
                pltpu.VMEM((T, 8 * 128), bf16),
                pltpu.VMEM((3, N8, D), bf16),
                pltpu.VMEM((N8, 2 * F), f32),
                pltpu.VMEM((N8, F), bf16),
                pltpu.VMEM((2, N8 // 2, D), bf16),
                pltpu.VMEM((2, N8 // 2, D), bf16),
                pltpu.VMEM((N8 // 2, D), f32),
                pltpu.VMEM((2, 6, T, half), bf16),
                pltpu.VMEM((2, 6, T, half), bf16),
                pltpu.VMEM((T, D), f32),
                pltpu.VMEM((2 * PAD, 128), f32),
                pltpu.VMEM((2 * PAD, 128), bf16),
                pltpu.VMEM((2 * PAD, 128), f32),
                pltpu.VMEM((2 * PAD, 128), f32),
                pltpu.VMEM((9 * 128, 256), bf16),
                pltpu.VMEM((wle.shape[0], 128), f32),
                pltpu.VMEM((1, 128), f32),
                pltpu.VMEM((N8, 128), f32),
                pltpu.VMEM((N8, 128), bf16),
                pltpu.VMEM((2, wq.shape[1], K), bf16),
                pltpu.VMEM((wls.shape[1], D), bf16),
                pltpu.VMEM(wle.shape, bf16),
                pltpu.VMEM((1, bias.shape[0]), f32),
                pltpu.VMEM((extra.shape[1], extra.shape[0]), f32),
                pltpu.VMEM((1, gain.shape[0]), f32),
                dma((3, 2, 2, n // 2)),
                dma((n // 2,)),
                dma((n // 2,)),
                dma((1,)),
                dma((2,)),
                dma((4, 3)),
                dma((5, 9)),
                dma((5,)),
                dma((2, CHUNKS, 4)),
                dma((2, 2)),
                dma((2,)),
                dma((2,)),
                dma((13,)),
            ],
            compiler_params=pltpu.CompilerParams(
                collective_id=0, has_side_effects=True, vmem_limit_bytes=60 * 1024 * 1024
            ),
        )(
            x, wsw, wex, wct, wq.T, wk.T, wv, wg, wls.T, wle, bias.reshape(1, -1), extra.T, gain.reshape(1, -1), wo
        )

    return jax.shard_map(
        per_device,
        mesh=mesh,
        in_specs=(
            P(("grp", "fs", "tp"), None),
            P("fs", "tp"),
            P("fs", "tp"),
            P("tp", "fs"),
            P("fs", "tp"),
            P("fs", "tp"),
            P("fs", "tp"),
            P("fs", "tp"),
            P(),
            P(None, "tp"),
            P("tp"),
            P(("grp", "fs"), "tp"),
            P(),
            P("tp", "fs"),
        ),
        out_specs=P(("grp", "fs", "tp"), None),
        check_vma=False,
    )
```

```python
import functools

import jax
import jax.numpy as jnp
from jax import lax
from jax.experimental import pallas as pl
from jax.experimental.pallas import tpu as pltpu
from jax.sharding import PartitionSpec as P

MESH = pl.DeviceIdType.MESH
DK = 64
DV = 128
SEQ = 320
PAD = 384
GAIN = 1.681792830507429
STEEP = 16.0
EPS = 1e-06
CHUNKS = 4
OFFSETS = (0, 2, 8, 0)
PAUSE, RESUME = 6, 13
NEAR = 5
FIRST = (
    "t0 w0 o0 m0", "w1 o1 m1 b0", "t0 b1 w2 o2", "m2 b2 w3 o3", "t0 m3 c0 c1", "b3 c2 g2 t0",
    "c3 d0 d1 t0", "d2 d3",
)
STEPS = ("o0 o1 m0 b0", "o2 m1 b1 o3", "m2 b2 m3 c0", "b3 c1 c2 c3", "d0 d1 d2 d3")
RIGHT, LEFT = 0, 1
A, B = 0, 1
f32, bf16 = jnp.float32, jnp.bfloat16


def mo(v, m):
    return pl.multiple_of(v, m)


def dot(a, b):
    return jnp.dot(a, b, preferred_element_type=f32)


def dot_t(a, b):
    return lax.dot_general(a, b, (((1,), (1,)), ((), ())), preferred_element_type=f32)


def kernel(
    n,
    x_in, wsw, wex, wct, wq_t, wk_t, wv, wg, wls_t, wle_in, bias_in, extra_t, gain_in, wo,
    out,
    gu, dn, qb, wof, ga, xg, acc, hb, pp, rp, sm, st, rt, br,
    qk, vb, og, lg, mm, wle2, bias2, extra2, gt,
    wqk, wls, wle, bias, extra, gain,
    z_recv, c_gu, c_dn, c_qb, c_ob, z_send, ag_recv, ag_send, rs_recv, rs_send, aa_recv, aa_send, loc,
):
    T, D = x_in.shape
    K = wsw.shape[0]
    F = wsw.shape[1]
    H = n // 2
    zi = lax.axis_index("fs")
    gi = lax.axis_index("grp")
    ti = lax.axis_index("tp")
    par = lax.rem(gi, 2)
    ci = lax.rem(ti, 2)
    xi = lax.div(ti, 2)
    oc = 1 - ci
    x1 = lax.rem(xi + 1, 4)
    x2 = lax.rem(xi + 2, 4)
    x3 = lax.rem(xi + 3, 4)
    z_right = {"fs": lax.rem(zi + 1, n)}
    z_left = {"fs": lax.rem(zi + n - 1, n)}
    y_dev = {"grp": gi + 1 - 2 * par}
    x_right = {"tp": x1 * 2 + ci}
    x_left = {"tp": x3 * 2 + ci}
    mate = {"tp": xi * 2 + oc}
    z_dev = (z_right, z_left)

    def remote(src, dst, s, r, dev):
        return pltpu.make_async_remote_copy(
            src_ref=src, dst_ref=dst, send_sem=s, recv_sem=r, device_id=dev, device_id_type=MESH
        )

    barrier = pltpu.get_barrier_semaphore()
    others = [{"tp": xx * 2 + cc} for xx in (x1, x2, x3) for cc in (ci, oc)]
    for dev in (z_right, z_left, y_dev, mate, *others):
        pl.semaphore_signal(barrier, inc=1, device_id=dev, device_id_type=MESH)

    locals_ = []
    own = pl.ds(mo(zi * K, K), K)
    for j in range(F // 128):
        col = slice(j * 128, j * 128 + 128)
        pltpu.make_async_copy(wsw.at[:, col], gu.at[own, pl.ds(j * 256, 128)], loc.at[12]).start()
        pltpu.make_async_copy(wex.at[:, col], gu.at[own, pl.ds(j * 256 + 128, 128)], loc.at[12]).start()
    locals_.append((x_in, xg.at[0, pl.ds(mo((ci * 4 + xi) * T, 16), T)]))
    locals_.append((wo, wof.at[pl.ds(mo(ti * 128, 128), 128), pl.ds(NEAR * K, K)]))
    first = len(locals_)
    locals_.append((wct, dn.at[:, own]))
    locals_.append((wv, qb.at[own, pl.ds(128, 128)]))
    locals_.append((wg, qb.at[own, pl.ds(256, 128)]))
    locals_.append((wq_t, wqk.at[0]))
    locals_.append((wk_t, wqk.at[1]))
    locals_ += [(wls_t, wls), (wle_in, wle), (bias_in, bias), (extra_t, extra), (gain_in, gain)]
    locals_ = [pltpu.make_async_copy(src, dst, loc.at[i]) for i, (src, dst) in enumerate(locals_)]
    for c in locals_:
        c.start()
    for c in locals_[:first]:
        c.wait()
    pltpu.make_async_copy(gu.at[own], gu.at[own], loc.at[12]).wait()
    pl.semaphore_wait(barrier, 10)

    def rows_of(o):
        return pl.ds(mo(o * K, K), K)

    def gu_at(o, ch):
        return gu.at[rows_of(o), pl.ds(mo(par * 896, 128), 384) if ch == A else pl.ds(384, 512)]

    def dn_at(o, ch):
        return dn.at[pl.ds(mo(par * 416, 16), 224) if ch == A else pl.ds(224, 192), rows_of(o)]

    def qb_at(o, ch):
        return qb.at[pl.ds(mo(o * K + par * (K // 2), K // 2), K // 2), 0:384]

    def ob_at(slot, ch):
        rows = mo(ti * 128 + par * 80, 16) if ch == A else mo(ti * 128 + 48, 16)
        return wof.at[pl.ds(rows, 48 if ch == A else 32), pl.ds(slot * K, K)]

    def ob_slot(d, dist):
        return (NEAR - dist) % n if d == RIGHT else (NEAR + dist) % n

    at = (gu_at, dn_at, qb_at, ob_at)
    R = (n - 1) * K
    whole = (
        (gu.at[0:R, 0:384], gu.at[0:R, 384:896]),
        (dn.at[0:224, 0:R], dn.at[224:416, 0:R]),
        (qb.at[0 : R // 2, 0:384], None),
        (wof.at[0:48, 0:R], wof.at[48:80, 0:R]),
    )

    def steps_of(ch, d):
        return H if (ch == A) == (d == RIGHT) else H - 1

    def origin(d, back):
        return lax.rem(zi + n - back, n) if d == RIGHT else lax.rem(zi + back, n)

    def z_copy(m, ch, d, s, o):
        if m == 3:
            src, dst = ob_at(ob_slot(d, s - 1), ch), ob_at(ob_slot(d, s), ch)
        else:
            src = dst = at[m](o, ch)
        return remote(src, dst, z_send.at[m, ch], z_recv.at[(0, 1, 0, 2)[m], d, ch, s - 1], z_dev[d])

    def tick(t):
        for m in range(4):
            s = t - OFFSETS[m]
            if m == 3 and t > PAUSE:
                s = t - RESUME + PAUSE + 1
                if s <= PAUSE:
                    continue
            if s < 1 or s > H + 1:
                continue
            for ch, d in ((A, RIGHT), (A, LEFT), (B, RIGHT), (B, LEFT)):
                last = steps_of(ch, d)
                if s - 1 > last or (m == 2 and ch == B):
                    continue
                o = origin(d, s - 1)
                if s > 1:
                    z_copy(m, ch, d, s - 1, o).wait_recv()
                if s <= last:
                    z_copy(m, ch, d, s, o).start()
                if s > 1 and ch == A:
                    ref = ob_at(ob_slot(d, s - 1), A) if m == 3 else at[m](o, A)
                    landed = (c_gu.at[s - 2], c_dn.at[s - 2], c_qb.at[0], c_ob.at[0 if s - 1 <= NEAR else 1])[m]
                    remote(ref, ref, z_send.at[m, 2], landed, y_dev).start()

    def qb_done():
        w = whole[2][A]
        remote(w, w, z_send.at[2, 2], c_qb.at[0], y_dev).wait_recv()

    def gu_done(dist):
        ref = gu.at[0 : (2 if dist < H else 1) * K, 0:384]
        remote(ref, ref, z_send.at[0, 2], c_gu.at[dist - 1], y_dev).wait_recv()

    def dn_done(dist):
        ref = dn.at[0:224, 0 : (2 if dist < H else 1) * K]
        remote(ref, ref, z_send.at[1, 2], c_dn.at[dist - 1], y_dev).wait_recv()

    def ob_done(batch):
        ref = wof.at[0:48, 0 : (2 * NEAR if batch == 0 else n - 1 - 2 * NEAR) * K]
        remote(ref, ref, z_send.at[3, 2], c_ob.at[batch], y_dev).wait_recv()

    def z_sent(m):
        for ch, i in ((A, A), (B, B), (A, 2)):
            w = whole[m][ch]
            if w is None:
                continue
            remote(w, w, z_send.at[m, i], c_qb.at[0], y_dev).wait_send()

    H0, H1 = pl.ds(0, D // 2), pl.ds(D // 2, D // 2)
    every = pl.ds(0, D)

    near_cols = (2 * NEAR + 1) * K
    batches = ((0, 6 * K, near_cols), (near_cols, near_cols + 3 * K, D))

    def ag(ph, i, xx, cc, cols, dev):
        if ph < 3:
            ref = xg.at[ph, pl.ds(mo((cc * 4 + xx) * T, 16), T), cols]
        else:
            lo, mid, hi = batches[ph - 3]
            cols = pl.ds(lo, mid - lo) if cols is H0 else pl.ds(mid, hi - mid) if cols is H1 else pl.ds(lo, hi - lo)
            ref = wof.at[pl.ds(mo((xx * 2 + cc) * 128, 128), 128), cols]
        slot = i if i < 7 else 8 if i in (9, 12) else 7
        return remote(ref, ref, ag_send.at[ph], ag_recv.at[ph, slot], dev)

    def from_mate(ph, slot, count):
        rows = count * (T if ph < 3 else 128)
        ref = xg.at[ph, 0:rows] if ph < 3 else wof.at[0:rows, batches[ph - 3][0] : batches[ph - 3][2]]
        remote(ref, ref, ag_send.at[ph], ag_recv.at[ph, slot], mate).wait_recv()

    def ag_start(ph):
        ag(ph, 0, xi, ci, H0, x_right).start()
        ag(ph, 3, xi, ci, H1, x_left).start()
        ag(ph, 6, xi, ci, every, mate).start()
        ag(ph, 1, xi, ci, H1, x_right).start()
        ag(ph, 4, xi, ci, H0, x_left).start()

    def ag_mid(ph):
        ag(ph, 0, x3, ci, H0, x_right).wait_recv()
        ag(ph, 2, x3, ci, H0, x_right).start()
        ag(ph, 7, x3, ci, H0, mate).start()
        ag(ph, 3, x1, ci, H1, x_left).wait_recv()
        ag(ph, 5, x1, ci, H1, x_left).start()
        ag(ph, 10, x1, ci, H1, mate).start()

    def ag_near(ph):
        ag(ph, 1, x3, ci, H1, x_right).wait_recv()
        ag(ph, 8, x3, ci, H1, mate).start()
        ag(ph, 4, x1, ci, H0, x_left).wait_recv()
        ag(ph, 11, x1, ci, H0, mate).start()
        if ph < 3:
            ag_near_mate(ph)

    def ag_near_mate(ph):
        if ph != 2:
            from_mate(ph, 6, 1)
        from_mate(ph, 7, 2)

    def ag_far(ph):
        ag(ph, 2, x2, ci, H0, x_right).wait_recv()
        ag(ph, 9, x2, ci, H0, mate).start()
        ag(ph, 5, x2, ci, H1, x_left).wait_recv()
        ag(ph, 12, x2, ci, H1, mate).start()

    def ag_end(ph):
        from_mate(ph, 8, 1)

    def ag_sent(ph):
        ref = xg.at[ph, 0 : 7 * T] if ph < 3 else wof.at[0 : 7 * 128, batches[ph - 3][0] : batches[ph - 3][2]]
        remote(ref, ref, ag_send.at[ph], ag_recv.at[ph, 0], mate).wait_send()

    W = D // CHUNKS
    V = W // 2

    def rs(ph, k, i, dev):
        if i == 6:
            src, dst = pp.at[ph, :, pl.ds(k * W, W)], rp.at[ph, :, pl.ds(k * W, W)]
        else:
            src, dst = st.at[ph, i, :, pl.ds(k * V, V)], rt.at[ph, i, :, pl.ds(k * V, V)]
        return remote(src, dst, rs_send.at[ph, i // 6], rs_recv.at[ph, k, (0, 2, 2, 1, 2, 2, 3)[i]], dev)

    rs_dev = (x_right, x_right, x_right, x_left, x_left, x_left, mate)
    my_rows = pl.ds(mo(ci * 4 * T, 16), 4 * T)
    mate_rows = pl.ds(mo(oc * 4 * T, 16), 4 * T)

    order = [(0, RIGHT)] + [(j // 2 + 1, j % 2) for j in range(n - 1)]
    BLOCKS = W // K

    def columns(ph, slot):
        if ph == 0:
            dist, d = order[slot]
            return pl.ds(mo(origin(d, dist) * K, K), K)
        return pl.ds(slot * K, K)

    def two_blocks(ph, wt, slot):
        if ph == 0:
            return jnp.concatenate([wt[:, columns(ph, slot)], wt[:, columns(ph, slot + 1)]], axis=1)
        return wt[:, pl.ds(slot * K, 2 * K)]

    def rs_o(ph, k, hid, wt):
        for slot in range(k * BLOCKS, (k + 1) * BLOCKS, 2):
            pp[ph, :, pl.ds(slot * K, 2 * K)] = dot(hid[mate_rows, :], two_blocks(ph, wt, slot)).astype(bf16)
        rs(ph, k, 6, mate).start()

    def rs_m(ph, k, hid, wt):
        for slot in range(k * BLOCKS, (k + 1) * BLOCKS, 2):
            sm[:, pl.ds(slot * K, 2 * K)] = dot(hid[my_rows, :], two_blocks(ph, wt, slot))

    def part(ph, xx, c0):
        rows, cols = pl.ds(mo(xx * T, 16), T), pl.ds(c0, V)
        return sm[rows, cols] + rp[ph, rows, cols].astype(f32)

    def rs_b(ph, k):
        rs(ph, k, 6, mate).wait_recv()
        lo, hi, to = k * W, k * W + V, pl.ds(k * V, V)
        for i, xx, c0 in ((0, x2, lo), (3, x2, hi), (1, x1, hi), (4, x3, lo)):
            st[ph, i, :, to] = part(ph, xx, c0).astype(bf16)
            rs(ph, k, i, rs_dev[i]).start()

    def rs_c(ph, k):
        lo, hi, to = k * W, k * W + V, pl.ds(k * V, V)
        for i, xx, c0 in ((0, x1, lo), (3, x3, hi)):
            rs(ph, k, i, rs_dev[i]).wait_recv()
            st[ph, i + 2, :, to] = (part(ph, xx, c0) + rt[ph, i, :, to].astype(f32)).astype(bf16)
            rs(ph, k, i + 2, rs_dev[i + 2]).start()

    def rs_d(ph, k):
        lo, hi, to = k * W, k * W + V, pl.ds(k * V, V)
        ref = rt.at[ph, 0:4, :, pl.ds(0, V)]
        remote(ref, ref, rs_send.at[ph, 0], rs_recv.at[ph, k, 2], mate).wait_recv()
        low = part(ph, xi, lo) + rt[ph, 2, :, to].astype(f32) + rt[ph, 4, :, to].astype(f32)
        high = part(ph, xi, hi) + rt[ph, 1, :, to].astype(f32) + rt[ph, 5, :, to].astype(f32)
        for i in range(BLOCKS // 2):
            br[:, columns(ph, k * BLOCKS + i)] = low[:, i * K : i * K + K]
            br[:, columns(ph, k * BLOCKS + BLOCKS // 2 + i)] = high[:, i * K : i * K + K]

    def rs_sent(ph):
        for i, ref in ((0, st.at[ph]), (1, pp.at[ph])):
            remote(ref, ref, rs_send.at[ph, i], rs_recv.at[ph, 0, 0], mate).wait_send()

    def run(ph, hid, wt, steps, clock=None):
        for step in " ".join(steps).split():
            what, k = step[0], int(step[1:])
            with jax.named_scope(f"rs{ph}_{step}"):
                if what in "wteg":
                    clock(what, k)
                elif what == "o":
                    rs_o(ph, k, hid, wt)
                elif what == "m":
                    rs_m(ph, k, hid, wt)
                else:
                    {"b": rs_b, "c": rs_c, "d": rs_d}[what](ph, k)

    own_rows = pl.ds(mo((ci * 4 + xi) * T, 16), T)

    def post_norm(ph, scale):
        z = GAIN * xg[ph, own_rows, :].astype(f32) + scale * br[...]
        z = z - jnp.mean(z, axis=-1, keepdims=True)
        return (z * lax.rsqrt(jnp.mean(z * z, axis=-1, keepdims=True) + EPS)).astype(bf16)

    def rows_at(cc, xx):
        return pl.ds(mo((cc * 4 + xx) * T, 16), T)

    def expand(ph, j0, j1, chips):
        where = [rows_at(cc, xx) for xx in chips for cc in (0, 1)]

        def one(j, _):
            w = gu[:, pl.ds(mo(j * 256, 256), 256)]
            to = pl.ds(mo(j * 128, 128), 128)
            p = dot(jnp.concatenate([xg[ph, r, :] for r in where], axis=0), w)
            gate, up = p[:, 0:128], p[:, 128:256]
            h = (gate / (1.0 + jnp.exp(-gate)) * up).astype(bf16)
            for i, r in enumerate(where):
                hb[r, to] = h[i * T : i * T + T, :]
            return 0

        lax.fori_loop(j0, j1, one, 0)

    def accumulate(o1, o2, first=False, last=False):
        def one(j, _):
            cols = pl.ds(mo(j * 256, 256), 256)
            w = jnp.concatenate([gu[rows_of(o1), cols], gu[rows_of(o2), cols]], axis=0)
            p = dot(jnp.concatenate([xg[0, :, rows_of(o1)], xg[0, :, rows_of(o2)]], axis=1), w)
            if not first:
                p = p + acc[:, cols]
            if last:
                gate, up = p[:, 0:128], p[:, 128:256]
                hb[:, pl.ds(mo(j * 128, 128), 128)] = (gate / (1.0 + jnp.exp(-gate)) * up).astype(bf16)
            else:
                acc[:, cols] = p
            return 0

        lax.fori_loop(0, F // 128, one, 0)

    def expand_pair(dist):
        with jax.named_scope(f"pair_{dist}"):
            gu_done(dist)
            if dist == H:
                accumulate(zi, origin(LEFT, H), last=True)
            else:
                accumulate(origin(RIGHT, dist), origin(LEFT, dist), first=dist == 1)

    def setup_attention():
        t = lax.broadcasted_iota(jnp.int32, (128, 256), 0)
        l = lax.broadcasted_iota(jnp.int32, (128, 256), 1)
        is_key = jnp.where(l >= 128, 1, 0)
        s = l - 128 * is_key
        before = (s + is_key) <= t
        after = (s - is_key) >= t
        for p in range(9):
            if p < 7:
                same = (t >> p) == (s >> p)
                odd = ((t >> p) & 1) == 1
                take = same & ((odd & before) | (jnp.logical_not(odd) & after))
            else:
                take = before if p == 7 else after
            mm[p * 128 : p * 128 + 128, :] = jnp.where(take, 1.0, 0.0).astype(bf16)
        for ref in (qk, lg, og, vb):
            for b in range(2):
                ref[b * PAD + SEQ : b * PAD + PAD, :] = jnp.zeros((PAD - SEQ, 128), ref.dtype)
        for h in range(2):
            lanes = slice(h * 64, h * 64 + 64)
            wle2[:, lanes] = wle[...].astype(f32)
            bias2[:, lanes] = bias[...]
            qb[own, lanes] = wqk[h].astype(f32).T.astype(bf16)
        qb[:, 384:512] = jnp.zeros((D, 128), bf16)
        for i in range(D // 128):
            qb[i * 128 : i * 128 + 128, 384 : 384 + wls.shape[0]] = (
                wls[:, i * 128 : i * 128 + 128].astype(f32).T.astype(bf16)
            )
        for h in range(2):
            lanes = slice(h * 64, h * 64 + 64)
            for i in range(8 * T // 128):
                extra2[i * 128 : i * 128 + 128, lanes] = extra[:, i * 128 : i * 128 + 128].T

    def project(b):
        seq = [rows_at(i % 2, 2 * b + i // 2) for i in range(4)]
        a = jnp.concatenate([xg[1, r, :] for r in seq], axis=0)
        to = pl.ds(mo(b * PAD, 128), SEQ)
        p1 = dot(a, qb[:, 0:256])
        qk[to, :] = p1[:, 0:128].astype(bf16).astype(f32)
        vb[to, :] = p1[:, 128:256].astype(bf16)
        p2 = dot(a, qb[:, 256:512])
        og[to, :] = p2[:, 0:128].astype(bf16).astype(f32)
        low = p2[:, 128 : 128 + wls.shape[0]].astype(bf16)
        pre = dot(low, wle2[...].astype(bf16)) + bias2[...]
        decay = (jnp.minimum(pre, 0.0) - jnp.log1p(jnp.exp(-jnp.abs(pre)))) / STEEP
        lg[to, :] = decay + extra2[pl.ds(mo(b * SEQ, 16), SEQ), :]

    def attend(b):
        lane = lax.broadcasted_iota(jnp.int32, (128, 128), 1)
        row = lax.broadcasted_iota(jnp.int32, (128, 128), 0)
        is_q = lane < 64
        differ = row ^ lane

        def sequence():
            heads, tails, totals, vals, diag = [], [], [], [], []
            for c in range(3):
                rows = pl.ds(mo(b * PAD + c * 128, 128), 128)
                both = qk[rows, :]
                g = lg[rows, :]
                hi = g.astype(bf16)
                lo = (g - hi.astype(f32)).astype(bf16)
                zero = jnp.zeros_like(hi)
                top = jnp.concatenate([jnp.where(is_q, hi, zero), jnp.where(is_q, lo, zero)], axis=1)
                bot = jnp.concatenate([jnp.where(is_q, zero, hi), jnp.where(is_q, zero, lo)], axis=1)
                e = dot(mm[...], jnp.concatenate([top, bot], axis=0))
                e = e[:, 0:128] + e[:, 128:256]
                w = jnp.exp(e)

                def pair(scaled):
                    q = jnp.where(is_q, scaled, 0.0).astype(bf16)
                    return q, pltpu.roll(scaled, 64, 1).astype(bf16)

                scores = dot_t(*pair(both))
                for p in range(7):
                    scores = jnp.where(differ >= (1 << p), dot_t(*pair(both * w[p * 128 : p * 128 + 128])), scores)
                diag.append(scores)
                heads.append(pair(both * w[896:1024]))
                tails.append((both, w[1024:1152], e[1024:1152]))
                totals.append(jnp.sum(g, axis=0, keepdims=True))
                vals.append(vb[rows, :])
                if c == 2:
                    tail = [pair(tails[i][0] * tails[i][1]) for i in range(2)]
                    far = pair(tails[0][0] * jnp.exp(tails[0][2] + totals[1]))
            s01 = dot_t(tail[0][0], heads[1][1])
            s10 = dot_t(heads[1][0], tail[0][1])
            s12 = dot_t(tail[1][0], heads[2][1])
            s21 = dot_t(heads[2][0], tail[1][1])
            s02 = dot_t(far[0], heads[2][1])
            s20 = dot_t(heads[2][0], far[1])
            grid = ((diag[0], s01, s02), (s10, diag[1], s12), (s20, s21, diag[2]))
            for c in range(3):
                rows = pl.ds(mo(b * PAD + c * 128, 128), 128)
                o = sum(dot(grid[c][i].astype(bf16), vals[i]) for i in range(3))
                o = o * lax.rsqrt(jnp.mean(o * o, axis=-1, keepdims=True) + EPS) * gain[...]
                gate = og[rows, :]
                qk[rows, :] = o * (gate / (1.0 + jnp.exp(-gate)))

        sequence()
        for i in range(4):
            gt[rows_at(i % 2, 2 * b + i // 2), :] = qk[pl.ds(mo(b * PAD + i * T, 16), T), :].astype(bf16)

    my_cols = pl.ds(mo(ti * 128, 128), 128)

    def hand_out(i, targets):
        for xx, cc in targets:
            remote(gt.at[rows_at(cc, xx)], ga.at[:, my_cols], aa_send.at[i], aa_recv.at[i], {"tp": xx * 2 + cc}).start()

    def handed(i, count):
        ref = gt.at[0 : count * T]
        return remote(ref, ref, aa_send.at[i], aa_recv.at[i], mate)

    def emit(slots):
        for slot in slots:
            p = dot(ga[...], wof[:, slot * K : slot * K + 2 * K])
            for i in range(2):
                o = lax.rem(zi + n + slot + i - NEAR, n)
                br[:, rows_of(o)] = p[:, i * K : i * K + K]

    at_tick = [1]
    last_tick = max(OFFSETS) + H + 1
    scope = jax.named_scope

    def advance(upto):
        while at_tick[0] <= min(upto, last_tick):
            with scope(f"tick_{at_tick[0]}"):
                tick(at_tick[0])
            at_tick[0] += 1

    def landed(k):
        advance(OFFSETS[1] + 2 * k + 3)
        with scope("dn_done"):
            dn_done(2 * k + 1)
            dn_done(2 * k + 2)

    def more(count):
        advance(at_tick[0] + count - 1)

    advance(1)
    ag_start(0)
    for c in locals_[first:]:
        c.wait()
    with scope("setup"):
        setup_attention()
    advance(2)
    with scope("ag0_mid"):
        ag_mid(0)
    advance(3)
    with scope("ag0_near"):
        ag_near(0)
    with scope("ag0_far"):
        ag_far(0)
    advance(4)
    ag_end(0)
    advance(5)
    for dist in (1, 2, 3):
        expand_pair(dist)
    advance(6)
    expand_pair(4)
    advance(7)
    with scope("ob_near"):
        ob_done(0)
        ag_start(3)
    expand_pair(5)
    advance(8)
    with scope("ob_mid"):
        ag_mid(3)
    expand_pair(6)
    expand_pair(7)
    advance(9)
    expand_pair(8)

    def other(what, k):
        if what == "w":
            landed(k)
        elif what == "t":
            more(1)
        else:
            ag_near(3)
            ag_far(3)

    run(0, hb, dn, FIRST, other)
    with scope("norm"):
        xg[1, own_rows, :] = post_norm(0, 0.5)
    ag_start(1)
    z_sent(0)
    z_sent(1)
    ag_sent(0)
    more(2)
    with scope("ag1_mid"):
        ag_mid(1)
    advance(last_tick)
    with scope("ag1_near"):
        ag_near(1)
    with scope("qb_done"):
        ob_done(1)
        ag_start(4)
        qb_done()
    seq = lax.div(xi, 2)
    pair = xi + 1 - 2 * lax.rem(xi, 2)
    away = 2 * (1 - seq)
    with scope("project"):
        project(seq)
    with scope("ag1_far"):
        ag_far(1)
    with scope("attend"):
        attend(seq)
        hand_out(0, ((pair, ci), (pair, oc), (xi, oc)))
    with scope("ag1_end"):
        ag_end(1)
    with scope("project"):
        project(1 - seq)
    with scope("ob2_mid"):
        ag_mid(4)
    with scope("attend"):
        attend(1 - seq)
        hand_out(1, ((away, 0), (away, 1), (away + 1, 0), (away + 1, 1)))
    ga[:, my_cols] = gt[own_rows, :]
    with scope("ob2_far"):
        ag_near(4)
        ag_far(4)
        ag_near_mate(3)
        ag_end(3)
    with scope("handed"):
        handed(0, 3).wait_recv()
        handed(1, 4).wait_recv()
    with scope("emit"):
        emit(range(0, 2 * NEAR, 2))
    with scope("ob_end"):
        ag_near_mate(4)
        ag_end(4)
    with scope("emit"):
        emit(range(2 * NEAR, n, 2))
    with scope("norm"):
        xg[2, own_rows, :] = post_norm(1, 1.0)
    ag_start(2)
    z_sent(2)
    z_sent(3)
    rs_sent(0)
    for i in (1, 3, 4):
        ag_sent(i)
    handed(0, 3).wait_send()
    handed(1, 4).wait_send()
    with scope("expand_own"):
        from_mate(2, 6, 1)
        expand(2, 0, 5, (xi,))
    with scope("ag2_mid"):
        ag_mid(2)
    with scope("ag2_near"):
        ag_near(2)
    near = (x1, x3)
    with scope("expand_near"):
        expand(2, 0, 3, near)
    with scope("ag2_far"):
        ag_far(2)
    with scope("expand_near"):
        expand(2, 3, 5, near)
    with scope("ag2_end"):
        ag_end(2)
    with scope("expand_far"):
        expand(2, 0, 5, (x2,))
    run(1, hb, dn, STEPS)
    with scope("norm"):
        out[...] = post_norm(2, 0.5)
    with scope("sent"):
        ag_sent(2)
        rs_sent(1)


def solution(mesh):
    n = mesh.shape["fs"]
    assert mesh.shape["grp"] % 2 == 0 and n % 2 == 0 and mesh.shape["tp"] == 8

    def per_device(x, wsw, wex, wct, wq, wk, wv, wg, wls, wle, bias, extra, gain, wo):
        T, D = x.shape
        K, F = wsw.shape
        N8 = 8 * T
        half = D // 2
        vmem = pl.BlockSpec(memory_space=pltpu.VMEM)
        anywhere = pl.BlockSpec(memory_space=pl.ANY)
        dma = pltpu.SemaphoreType.DMA
        return pl.pallas_call(
            functools.partial(kernel, n),
            out_shape=jax.ShapeDtypeStruct((T, D), bf16),
            in_specs=[anywhere] * 14,
            out_specs=vmem,
            scratch_shapes=[
                pltpu.VMEM((D, 2 * F), bf16),
                pltpu.VMEM((F, D), bf16),
                pltpu.VMEM((D, 512), bf16),
                pltpu.VMEM((8 * 128, D), bf16),
                pltpu.VMEM((T, 8 * 128), bf16),
                pltpu.VMEM((3, N8, D), bf16),
                pltpu.VMEM((N8, 2 * F), f32),
                pltpu.VMEM((N8, F), bf16),
                pltpu.VMEM((2, N8 // 2, D), bf16),
                pltpu.VMEM((2, N8 // 2, D), bf16),
                pltpu.VMEM((N8 // 2, D), f32),
                pltpu.VMEM((2, 6, T, half), bf16),
                pltpu.VMEM((2, 6, T, half), bf16),
                pltpu.VMEM((T, D), f32),
                pltpu.VMEM((2 * PAD, 128), f32),
                pltpu.VMEM((2 * PAD, 128), bf16),
                pltpu.VMEM((2 * PAD, 128), f32),
                pltpu.VMEM((2 * PAD, 128), f32),
                pltpu.VMEM((9 * 128, 256), bf16),
                pltpu.VMEM((wle.shape[0], 128), f32),
                pltpu.VMEM((1, 128), f32),
                pltpu.VMEM((N8, 128), f32),
                pltpu.VMEM((N8, 128), bf16),
                pltpu.VMEM((2, wq.shape[1], K), bf16),
                pltpu.VMEM((wls.shape[1], D), bf16),
                pltpu.VMEM(wle.shape, bf16),
                pltpu.VMEM((1, bias.shape[0]), f32),
                pltpu.VMEM((extra.shape[1], extra.shape[0]), f32),
                pltpu.VMEM((1, gain.shape[0]), f32),
                dma((3, 2, 2, n // 2)),
                dma((n // 2,)),
                dma((n // 2,)),
                dma((1,)),
                dma((2,)),
                dma((4, 3)),
                dma((5, 9)),
                dma((5,)),
                dma((2, CHUNKS, 4)),
                dma((2, 2)),
                dma((2,)),
                dma((2,)),
                dma((13,)),
            ],
            compiler_params=pltpu.CompilerParams(
                collective_id=0, has_side_effects=True, vmem_limit_bytes=60 * 1024 * 1024
            ),
        )(
            x, wsw, wex, wct, wq.T, wk.T, wv, wg, wls.T, wle, bias.reshape(1, -1), extra.T, gain.reshape(1, -1), wo
        )

    return jax.shard_map(
        per_device,
        mesh=mesh,
        in_specs=(
            P(("grp", "fs", "tp"), None),
            P("fs", "tp"),
            P("fs", "tp"),
            P("tp", "fs"),
            P("fs", "tp"),
            P("fs", "tp"),
            P("fs", "tp"),
            P("fs", "tp"),
            P(),
            P(None, "tp"),
            P("tp"),
            P(("grp", "fs"), "tp"),
            P(),
            P("tp", "fs"),
        ),
        out_specs=P(("grp", "fs", "tp"), None),
        check_vma=False,
    )
```

```python
import functools

import jax
import jax.numpy as jnp
from jax import lax
from jax.experimental import pallas as pl
from jax.experimental.pallas import tpu as pltpu
from jax.sharding import PartitionSpec as P

MESH = pl.DeviceIdType.MESH
DK = 64
DV = 128
SEQ = 320
PAD = 384
GAIN = 1.681792830507429
STEEP = 16.0
EPS = 1e-06
CHUNKS = 4
OFFSETS = (0, 2, 8, 0)
PAUSE, RESUME = 6, 13
NEAR = 5
FIRST = (
    "t0 w0 o0 m0", "w1 o1 m1 b0", "t0 b1 w2 o2", "m2 b2 w3 o3", "t0 m3 c0 c1", "b3 c2 g2 t0",
    "c3 d0 d1 t0", "d2 d3",
)
STEPS = ("o0 o1 m0 b0", "o2 m1 b1 o3", "m2 b2 m3 c0", "b3 c1 c2 c3", "d0 d1 d2 d3")
RIGHT, LEFT = 0, 1
A, B = 0, 1
f32, bf16 = jnp.float32, jnp.bfloat16


def mo(v, m):
    return pl.multiple_of(v, m)


def dot(a, b):
    return jnp.dot(a, b, preferred_element_type=f32)


def dot_t(a, b):
    return lax.dot_general(a, b, (((1,), (1,)), ((), ())), preferred_element_type=f32)


def kernel(
    n,
    x_in, wsw, wex, wct, wq_t, wk_t, wv, wg, wls_t, wle_in, bias_in, extra_t, gain_in, wo,
    out,
    gu, dn, qb, wof, ga, xg, acc, hb, pp, rp, sm, st, rt, br,
    qk, vb, og, lg, mm, wle2, bias2, extra2, gt,
    wqk, wls, wle, bias, extra, gain,
    z_recv, c_gu, c_dn, c_qb, c_ob, z_send, ag_recv, ag_send, rs_recv, rs_send, aa_recv, aa_send, loc,
):
    T, D = x_in.shape
    K = wsw.shape[0]
    F = wsw.shape[1]
    H = n // 2
    zi = lax.axis_index("fs")
    gi = lax.axis_index("grp")
    ti = lax.axis_index("tp")
    par = lax.rem(gi, 2)
    ci = lax.rem(ti, 2)
    xi = lax.div(ti, 2)
    oc = 1 - ci
    x1 = lax.rem(xi + 1, 4)
    x2 = lax.rem(xi + 2, 4)
    x3 = lax.rem(xi + 3, 4)
    z_right = {"fs": lax.rem(zi + 1, n)}
    z_left = {"fs": lax.rem(zi + n - 1, n)}
    y_dev = {"grp": gi + 1 - 2 * par}
    x_right = {"tp": x1 * 2 + ci}
    x_left = {"tp": x3 * 2 + ci}
    mate = {"tp": xi * 2 + oc}
    z_dev = (z_right, z_left)

    def remote(src, dst, s, r, dev):
        return pltpu.make_async_remote_copy(
            src_ref=src, dst_ref=dst, send_sem=s, recv_sem=r, device_id=dev, device_id_type=MESH
        )

    barrier = pltpu.get_barrier_semaphore()
    others = [{"tp": xx * 2 + cc} for xx in (x1, x2, x3) for cc in (ci, oc)]
    for dev in (z_right, z_left, y_dev, mate, *others):
        pl.semaphore_signal(barrier, inc=1, device_id=dev, device_id_type=MESH)

    locals_ = []
    own = pl.ds(mo(zi * K, K), K)
    for j in range(F // 128):
        col = slice(j * 128, j * 128 + 128)
        pltpu.make_async_copy(wsw.at[:, col], gu.at[own, pl.ds(j * 256, 128)], loc.at[12]).start()
        pltpu.make_async_copy(wex.at[:, col], gu.at[own, pl.ds(j * 256 + 128, 128)], loc.at[12]).start()
    locals_.append((x_in, xg.at[0, pl.ds(mo((ci * 4 + xi) * T, 16), T)]))
    locals_.append((wo, wof.at[pl.ds(mo(ti * 128, 128), 128), pl.ds(NEAR * K, K)]))
    first = len(locals_)
    locals_.append((wct, dn.at[:, own]))
    locals_.append((wv, qb.at[own, pl.ds(128, 128)]))
    locals_.append((wg, qb.at[own, pl.ds(256, 128)]))
    locals_.append((wq_t, wqk.at[0]))
    locals_.append((wk_t, wqk.at[1]))
    locals_ += [(wls_t, wls), (wle_in, wle), (bias_in, bias), (extra_t, extra), (gain_in, gain)]
    locals_ = [pltpu.make_async_copy(src, dst, loc.at[i]) for i, (src, dst) in enumerate(locals_)]
    for c in locals_:
        c.start()
    for c in locals_[:first]:
        c.wait()
    pltpu.make_async_copy(gu.at[own], gu.at[own], loc.at[12]).wait()
    pl.semaphore_wait(barrier, 10)

    def rows_of(o):
        return pl.ds(mo(o * K, K), K)

    def gu_at(o, ch):
        return gu.at[rows_of(o), pl.ds(mo(par * 896, 128), 384) if ch == A else pl.ds(384, 512)]

    def dn_at(o, ch):
        return dn.at[pl.ds(mo(par * 416, 16), 224) if ch == A else pl.ds(224, 192), rows_of(o)]

    def qb_at(o, ch):
        return qb.at[pl.ds(mo(o * K + par * (K // 2), K // 2), K // 2), 0:384]

    def ob_at(slot, ch):
        return wof.at[pl.ds(mo(ti * 128 + par * 64, 64), 64), pl.ds(slot * K, K)]

    def ob_slot(d, dist):
        return (NEAR - dist) % n if d == RIGHT else (NEAR + dist) % n

    at = (gu_at, dn_at, qb_at, ob_at)
    R = (n - 1) * K
    whole = (
        (gu.at[0:R, 0:384], gu.at[0:R, 384:896]),
        (dn.at[0:224, 0:R], dn.at[224:416, 0:R]),
        (qb.at[0 : R // 2, 0:384], None),
        (wof.at[0:64, 0:R], None),
    )

    def steps_of(ch, d):
        return H if (ch == A) == (d == RIGHT) else H - 1

    def origin(d, back):
        return lax.rem(zi + n - back, n) if d == RIGHT else lax.rem(zi + back, n)

    def z_copy(m, ch, d, s, o):
        if m == 3:
            src, dst = ob_at(ob_slot(d, s - 1), ch), ob_at(ob_slot(d, s), ch)
        else:
            src = dst = at[m](o, ch)
        return remote(src, dst, z_send.at[m, ch], z_recv.at[(0, 2, 0, 4)[m] + ch, d, (s - 1) % 4], z_dev[d])

    def tick(t):
        for m in range(4):
            s = t - OFFSETS[m]
            if m == 3 and t > PAUSE:
                s = t - RESUME + PAUSE + 1
                if s <= PAUSE:
                    continue
            if s < 1 or s > H + 1:
                continue
            for ch, d in ((A, RIGHT), (A, LEFT), (B, RIGHT), (B, LEFT)):
                last = steps_of(ch, d)
                if s - 1 > last or (m >= 2 and ch == B):
                    continue
                o = origin(d, s - 1)
                if s > 1:
                    z_copy(m, ch, d, s - 1, o).wait_recv()
                if s <= last:
                    z_copy(m, ch, d, s, o).start()
                if s > 1 and ch == A:
                    ref = ob_at(ob_slot(d, s - 1), A) if m == 3 else at[m](o, A)
                    landed = (c_gu.at[s - 2], c_dn.at[s - 2], c_qb.at[0], c_ob.at[0 if s - 1 <= NEAR else 1])[m]
                    remote(ref, ref, z_send.at[m, 2], landed, y_dev).start()

    def qb_done():
        w = whole[2][A]
        remote(w, w, z_send.at[2, 2], c_qb.at[0], y_dev).wait_recv()

    def gu_done(dist):
        ref = gu.at[0 : (2 if dist < H else 1) * K, 0:384]
        remote(ref, ref, z_send.at[0, 2], c_gu.at[dist - 1], y_dev).wait_recv()

    def dn_done(dist):
        ref = dn.at[0:224, 0 : (2 if dist < H else 1) * K]
        remote(ref, ref, z_send.at[1, 2], c_dn.at[dist - 1], y_dev).wait_recv()

    def ob_done(batch):
        ref = wof.at[0:64, 0 : (2 * NEAR if batch == 0 else n - 1 - 2 * NEAR) * K]
        remote(ref, ref, z_send.at[3, 2], c_ob.at[batch], y_dev).wait_recv()

    def z_sent(m):
        for ch, i in ((A, A), (B, B), (A, 2)):
            w = whole[m][ch]
            if w is None:
                continue
            remote(w, w, z_send.at[m, i], c_qb.at[0], y_dev).wait_send()

    H0, H1 = pl.ds(0, D // 2), pl.ds(D // 2, D // 2)
    every = pl.ds(0, D)

    near_cols = (2 * NEAR + 1) * K
    batches = ((0, 6 * K, near_cols), (near_cols, near_cols + 3 * K, D))

    def ag(ph, i, xx, cc, cols, dev):
        if ph < 3:
            ref = xg.at[ph, pl.ds(mo((cc * 4 + xx) * T, 16), T), cols]
        else:
            lo, mid, hi = batches[ph - 3]
            cols = pl.ds(lo, mid - lo) if cols is H0 else pl.ds(mid, hi - mid) if cols is H1 else pl.ds(lo, hi - lo)
            ref = wof.at[pl.ds(mo((xx * 2 + cc) * 128, 128), 128), cols]
        slot = i if i < 7 else 8 if i in (9, 12) else 7
        return remote(ref, ref, ag_send.at[ph], ag_recv.at[ph, slot], dev)

    def from_mate(ph, slot, count):
        rows = count * (T if ph < 3 else 128)
        ref = xg.at[ph, 0:rows] if ph < 3 else wof.at[0:rows, batches[ph - 3][0] : batches[ph - 3][2]]
        remote(ref, ref, ag_send.at[ph], ag_recv.at[ph, slot], mate).wait_recv()

    def ag_start(ph):
        ag(ph, 0, xi, ci, H0, x_right).start()
        ag(ph, 3, xi, ci, H1, x_left).start()
        ag(ph, 6, xi, ci, every, mate).start()
        ag(ph, 1, xi, ci, H1, x_right).start()
        ag(ph, 4, xi, ci, H0, x_left).start()

    def ag_mid(ph):
        ag(ph, 0, x3, ci, H0, x_right).wait_recv()
        ag(ph, 2, x3, ci, H0, x_right).start()
        ag(ph, 7, x3, ci, H0, mate).start()
        ag(ph, 3, x1, ci, H1, x_left).wait_recv()
        ag(ph, 5, x1, ci, H1, x_left).start()
        ag(ph, 10, x1, ci, H1, mate).start()

    def ag_near(ph):
        ag(ph, 1, x3, ci, H1, x_right).wait_recv()
        ag(ph, 8, x3, ci, H1, mate).start()
        ag(ph, 4, x1, ci, H0, x_left).wait_recv()
        ag(ph, 11, x1, ci, H0, mate).start()
        if ph < 3:
            ag_near_mate(ph)

    def ag_near_mate(ph):
        if ph != 2:
            from_mate(ph, 6, 1)
        from_mate(ph, 7, 2)

    def ag_far(ph):
        ag(ph, 2, x2, ci, H0, x_right).wait_recv()
        ag(ph, 9, x2, ci, H0, mate).start()
        ag(ph, 5, x2, ci, H1, x_left).wait_recv()
        ag(ph, 12, x2, ci, H1, mate).start()

    def ag_end(ph):
        from_mate(ph, 8, 1)

    def ag_sent(ph):
        ref = xg.at[ph, 0 : 7 * T] if ph < 3 else wof.at[0 : 7 * 128, batches[ph - 3][0] : batches[ph - 3][2]]
        remote(ref, ref, ag_send.at[ph], ag_recv.at[ph, 0], mate).wait_send()

    W = D // CHUNKS
    V = W // 2

    def rs(ph, k, i, dev):
        if i == 6:
            src, dst = pp.at[ph, :, pl.ds(k * W, W)], rp.at[ph, :, pl.ds(k * W, W)]
        else:
            src, dst = st.at[ph, i, :, pl.ds(k * V, V)], rt.at[ph, i, :, pl.ds(k * V, V)]
        return remote(src, dst, rs_send.at[ph, i // 6], rs_recv.at[ph, k, (0, 2, 2, 1, 2, 2, 3)[i]], dev)

    rs_dev = (x_right, x_right, x_right, x_left, x_left, x_left, mate)
    my_rows = pl.ds(mo(ci * 4 * T, 16), 4 * T)
    mate_rows = pl.ds(mo(oc * 4 * T, 16), 4 * T)

    order = [(0, RIGHT)] + [(j // 2 + 1, j % 2) for j in range(n - 1)]
    BLOCKS = W // K

    def columns(ph, slot):
        if ph == 0:
            dist, d = order[slot]
            return pl.ds(mo(origin(d, dist) * K, K), K)
        return pl.ds(slot * K, K)

    def two_blocks(ph, wt, slot):
        if ph == 0:
            return jnp.concatenate([wt[:, columns(ph, slot)], wt[:, columns(ph, slot + 1)]], axis=1)
        return wt[:, pl.ds(slot * K, 2 * K)]

    def rs_o(ph, k, hid, wt):
        for slot in range(k * BLOCKS, (k + 1) * BLOCKS, 2):
            pp[ph, :, pl.ds(slot * K, 2 * K)] = dot(hid[mate_rows, :], two_blocks(ph, wt, slot)).astype(bf16)
        rs(ph, k, 6, mate).start()

    def rs_m(ph, k, hid, wt):
        for slot in range(k * BLOCKS, (k + 1) * BLOCKS, 2):
            sm[:, pl.ds(slot * K, 2 * K)] = dot(hid[my_rows, :], two_blocks(ph, wt, slot))

    def part(ph, xx, c0):
        rows, cols = pl.ds(mo(xx * T, 16), T), pl.ds(c0, V)
        return sm[rows, cols] + rp[ph, rows, cols].astype(f32)

    def rs_b(ph, k):
        rs(ph, k, 6, mate).wait_recv()
        lo, hi, to = k * W, k * W + V, pl.ds(k * V, V)
        for i, xx, c0 in ((0, x2, lo), (3, x2, hi), (1, x1, hi), (4, x3, lo)):
            st[ph, i, :, to] = part(ph, xx, c0).astype(bf16)
            rs(ph, k, i, rs_dev[i]).start()

    def rs_c(ph, k):
        lo, hi, to = k * W, k * W + V, pl.ds(k * V, V)
        for i, xx, c0 in ((0, x1, lo), (3, x3, hi)):
            rs(ph, k, i, rs_dev[i]).wait_recv()
            st[ph, i + 2, :, to] = (part(ph, xx, c0) + rt[ph, i, :, to].astype(f32)).astype(bf16)
            rs(ph, k, i + 2, rs_dev[i + 2]).start()

    def rs_d(ph, k):
        lo, hi, to = k * W, k * W + V, pl.ds(k * V, V)
        ref = rt.at[ph, 0:4, :, pl.ds(0, V)]
        remote(ref, ref, rs_send.at[ph, 0], rs_recv.at[ph, k, 2], mate).wait_recv()
        low = part(ph, xi, lo) + rt[ph, 2, :, to].astype(f32) + rt[ph, 4, :, to].astype(f32)
        high = part(ph, xi, hi) + rt[ph, 1, :, to].astype(f32) + rt[ph, 5, :, to].astype(f32)
        for i in range(BLOCKS // 2):
            br[:, columns(ph, k * BLOCKS + i)] = low[:, i * K : i * K + K]
            br[:, columns(ph, k * BLOCKS + BLOCKS // 2 + i)] = high[:, i * K : i * K + K]

    def rs_sent(ph):
        for i, ref in ((0, st.at[ph]), (1, pp.at[ph])):
            remote(ref, ref, rs_send.at[ph, i], rs_recv.at[ph, 0, 0], mate).wait_send()

    def run(ph, hid, wt, steps, clock=None):
        for step in " ".join(steps).split():
            what, k = step[0], int(step[1:])
            with jax.named_scope(f"rs{ph}_{step}"):
                if what in "wteg":
                    clock(what, k)
                elif what == "o":
                    rs_o(ph, k, hid, wt)
                elif what == "m":
                    rs_m(ph, k, hid, wt)
                else:
                    {"b": rs_b, "c": rs_c, "d": rs_d}[what](ph, k)

    own_rows = pl.ds(mo((ci * 4 + xi) * T, 16), T)

    def post_norm(ph, scale):
        z = GAIN * xg[ph, own_rows, :].astype(f32) + scale * br[...]
        z = z - jnp.mean(z, axis=-1, keepdims=True)
        return (z * lax.rsqrt(jnp.mean(z * z, axis=-1, keepdims=True) + EPS)).astype(bf16)

    def rows_at(cc, xx):
        return pl.ds(mo((cc * 4 + xx) * T, 16), T)

    def expand(ph, j0, j1, chips):
        where = [rows_at(cc, xx) for xx in chips for cc in (0, 1)]

        def one(j, _):
            w = gu[:, pl.ds(mo(j * 256, 256), 256)]
            to = pl.ds(mo(j * 128, 128), 128)
            p = dot(jnp.concatenate([xg[ph, r, :] for r in where], axis=0), w)
            gate, up = p[:, 0:128], p[:, 128:256]
            h = (gate / (1.0 + jnp.exp(-gate)) * up).astype(bf16)
            for i, r in enumerate(where):
                hb[r, to] = h[i * T : i * T + T, :]
            return 0

        lax.fori_loop(j0, j1, one, 0)

    def accumulate(o1, o2, first=False, last=False):
        def one(j, _):
            cols = pl.ds(mo(j * 256, 256), 256)
            w = jnp.concatenate([gu[rows_of(o1), cols], gu[rows_of(o2), cols]], axis=0)
            p = dot(jnp.concatenate([xg[0, :, rows_of(o1)], xg[0, :, rows_of(o2)]], axis=1), w)
            if not first:
                p = p + acc[:, cols]
            if last:
                gate, up = p[:, 0:128], p[:, 128:256]
                hb[:, pl.ds(mo(j * 128, 128), 128)] = (gate / (1.0 + jnp.exp(-gate)) * up).astype(bf16)
            else:
                acc[:, cols] = p
            return 0

        lax.fori_loop(0, F // 128, one, 0)

    def expand_pair(dist):
        with jax.named_scope(f"pair_{dist}"):
            gu_done(dist)
            if dist == H:
                accumulate(zi, origin(LEFT, H), last=True)
            else:
                accumulate(origin(RIGHT, dist), origin(LEFT, dist), first=dist == 1)

    def setup_attention():
        t = lax.broadcasted_iota(jnp.int32, (128, 256), 0)
        l = lax.broadcasted_iota(jnp.int32, (128, 256), 1)
        is_key = jnp.where(l >= 128, 1, 0)
        s = l - 128 * is_key
        before = (s + is_key) <= t
        after = (s - is_key) >= t
        for p in range(9):
            if p < 7:
                same = (t >> p) == (s >> p)
                odd = ((t >> p) & 1) == 1
                take = same & ((odd & before) | (jnp.logical_not(odd) & after))
            else:
                take = before if p == 7 else after
            mm[p * 128 : p * 128 + 128, :] = jnp.where(take, 1.0, 0.0).astype(bf16)
        for ref in (qk, lg, og, vb):
            for b in range(2):
                ref[b * PAD + SEQ : b * PAD + PAD, :] = jnp.zeros((PAD - SEQ, 128), ref.dtype)
        for h in range(2):
            lanes = slice(h * 64, h * 64 + 64)
            wle2[:, lanes] = wle[...].astype(f32)
            bias2[:, lanes] = bias[...]
            qb[own, lanes] = wqk[h].astype(f32).T.astype(bf16)
        qb[:, 384:512] = jnp.zeros((D, 128), bf16)
        for i in range(D // 128):
            qb[i * 128 : i * 128 + 128, 384 : 384 + wls.shape[0]] = (
                wls[:, i * 128 : i * 128 + 128].astype(f32).T.astype(bf16)
            )
        for h in range(2):
            lanes = slice(h * 64, h * 64 + 64)
            for i in range(8 * T // 128):
                extra2[i * 128 : i * 128 + 128, lanes] = extra[:, i * 128 : i * 128 + 128].T

    def project(b):
        seq = [rows_at(i % 2, 2 * b + i // 2) for i in range(4)]
        a = jnp.concatenate([xg[1, r, :] for r in seq], axis=0)
        to = pl.ds(mo(b * PAD, 128), SEQ)
        p1 = dot(a, qb[:, 0:256])
        qk[to, :] = p1[:, 0:128].astype(bf16).astype(f32)
        vb[to, :] = p1[:, 128:256].astype(bf16)
        p2 = dot(a, qb[:, 256:512])
        og[to, :] = p2[:, 0:128].astype(bf16).astype(f32)
        low = p2[:, 128 : 128 + wls.shape[0]].astype(bf16)
        pre = dot(low, wle2[...].astype(bf16)) + bias2[...]
        decay = (jnp.minimum(pre, 0.0) - jnp.log1p(jnp.exp(-jnp.abs(pre)))) / STEEP
        lg[to, :] = decay + extra2[pl.ds(mo(b * SEQ, 16), SEQ), :]

    def attend(b):
        lane = lax.broadcasted_iota(jnp.int32, (128, 128), 1)
        row = lax.broadcasted_iota(jnp.int32, (128, 128), 0)
        is_q = lane < 64
        differ = row ^ lane

        def sequence():
            heads, tails, totals, vals, diag = [], [], [], [], []
            for c in range(3):
                rows = pl.ds(mo(b * PAD + c * 128, 128), 128)
                both = qk[rows, :]
                g = lg[rows, :]
                hi = g.astype(bf16)
                lo = (g - hi.astype(f32)).astype(bf16)
                zero = jnp.zeros_like(hi)
                top = jnp.concatenate([jnp.where(is_q, hi, zero), jnp.where(is_q, lo, zero)], axis=1)
                bot = jnp.concatenate([jnp.where(is_q, zero, hi), jnp.where(is_q, zero, lo)], axis=1)
                e = dot(mm[...], jnp.concatenate([top, bot], axis=0))
                e = e[:, 0:128] + e[:, 128:256]
                w = jnp.exp(e)

                def pair(scaled):
                    q = jnp.where(is_q, scaled, 0.0).astype(bf16)
                    return q, pltpu.roll(scaled, 64, 1).astype(bf16)

                scores = dot_t(*pair(both))
                for p in range(7):
                    scores = jnp.where(differ >= (1 << p), dot_t(*pair(both * w[p * 128 : p * 128 + 128])), scores)
                diag.append(scores)
                heads.append(pair(both * w[896:1024]))
                tails.append((both, w[1024:1152], e[1024:1152]))
                totals.append(jnp.sum(g, axis=0, keepdims=True))
                vals.append(vb[rows, :])
                if c == 2:
                    tail = [pair(tails[i][0] * tails[i][1]) for i in range(2)]
                    far = pair(tails[0][0] * jnp.exp(tails[0][2] + totals[1]))
            s01 = dot_t(tail[0][0], heads[1][1])
            s10 = dot_t(heads[1][0], tail[0][1])
            s12 = dot_t(tail[1][0], heads[2][1])
            s21 = dot_t(heads[2][0], tail[1][1])
            s02 = dot_t(far[0], heads[2][1])
            s20 = dot_t(heads[2][0], far[1])
            grid = ((diag[0], s01, s02), (s10, diag[1], s12), (s20, s21, diag[2]))
            for c in range(3):
                rows = pl.ds(mo(b * PAD + c * 128, 128), 128)
                o = sum(dot(grid[c][i].astype(bf16), vals[i]) for i in range(3))
                o = o * lax.rsqrt(jnp.mean(o * o, axis=-1, keepdims=True) + EPS) * gain[...]
                gate = og[rows, :]
                qk[rows, :] = o * (gate / (1.0 + jnp.exp(-gate)))

        sequence()
        for i in range(4):
            gt[rows_at(i % 2, 2 * b + i // 2), :] = qk[pl.ds(mo(b * PAD + i * T, 16), T), :].astype(bf16)

    my_cols = pl.ds(mo(ti * 128, 128), 128)

    def hand_out(i, targets):
        for xx, cc in targets:
            remote(gt.at[rows_at(cc, xx)], ga.at[:, my_cols], aa_send.at[i], aa_recv.at[i], {"tp": xx * 2 + cc}).start()

    def handed(i, count):
        ref = gt.at[0 : count * T]
        return remote(ref, ref, aa_send.at[i], aa_recv.at[i], mate)

    def emit(slots):
        for slot in slots:
            p = dot(ga[...], wof[:, slot * K : slot * K + 2 * K])
            for i in range(2):
                o = lax.rem(zi + n + slot + i - NEAR, n)
                br[:, rows_of(o)] = p[:, i * K : i * K + K]

    at_tick = [1]
    last_tick = max(OFFSETS) + H + 1
    scope = jax.named_scope

    def advance(upto):
        while at_tick[0] <= min(upto, last_tick):
            with scope(f"tick_{at_tick[0]}"):
                tick(at_tick[0])
            at_tick[0] += 1

    def landed(k):
        advance(OFFSETS[1] + 2 * k + 3)
        with scope("dn_done"):
            dn_done(2 * k + 1)
            dn_done(2 * k + 2)

    def more(count):
        advance(at_tick[0] + count - 1)

    advance(1)
    ag_start(0)
    for c in locals_[first:]:
        c.wait()
    with scope("setup"):
        setup_attention()
    advance(2)
    with scope("ag0_mid"):
        ag_mid(0)
    advance(3)
    with scope("ag0_near"):
        ag_near(0)
    with scope("ag0_far"):
        ag_far(0)
    advance(4)
    ag_end(0)
    advance(5)
    for dist in (1, 2, 3):
        expand_pair(dist)
    advance(6)
    expand_pair(4)
    advance(7)
    with scope("ob_near"):
        ob_done(0)
        ag_start(3)
    expand_pair(5)
    advance(8)
    with scope("ob_mid"):
        ag_mid(3)
    expand_pair(6)
    expand_pair(7)
    advance(9)
    expand_pair(8)

    def other(what, k):
        if what == "w":
            landed(k)
        elif what == "t":
            more(1)
        else:
            ag_near(3)
            ag_far(3)

    run(0, hb, dn, FIRST, other)
    with scope("norm"):
        xg[1, own_rows, :] = post_norm(0, 0.5)
    ag_start(1)
    z_sent(0)
    z_sent(1)
    ag_sent(0)
    more(2)
    with scope("ag1_mid"):
        ag_mid(1)
    advance(last_tick)
    with scope("ag1_near"):
        ag_near(1)
    with scope("qb_done"):
        ob_done(1)
        ag_start(4)
        qb_done()
    seq = lax.div(xi, 2)
    pair = xi + 1 - 2 * lax.rem(xi, 2)
    away = 2 * (1 - seq)
    with scope("project"):
        project(seq)
    with scope("ag1_far"):
        ag_far(1)
    with scope("attend"):
        attend(seq)
        hand_out(0, ((pair, ci), (pair, oc), (xi, oc)))
    with scope("ag1_end"):
        ag_end(1)
    with scope("project"):
        project(1 - seq)
    with scope("ob2_mid"):
        ag_mid(4)
    with scope("attend"):
        attend(1 - seq)
        hand_out(1, ((away, 0), (away, 1), (away + 1, 0), (away + 1, 1)))
    ga[:, my_cols] = gt[own_rows, :]
    with scope("ob2_far"):
        ag_near(4)
        ag_far(4)
        ag_near_mate(3)
        ag_end(3)
    with scope("handed"):
        handed(0, 3).wait_recv()
        handed(1, 4).wait_recv()
    with scope("emit"):
        emit(range(0, 2 * NEAR, 2))
    with scope("ob_end"):
        ag_near_mate(4)
        ag_end(4)
    with scope("emit"):
        emit(range(2 * NEAR, n, 2))
    with scope("norm"):
        xg[2, own_rows, :] = post_norm(1, 1.0)
    ag_start(2)
    z_sent(2)
    z_sent(3)
    rs_sent(0)
    for i in (1, 3, 4):
        ag_sent(i)
    handed(0, 3).wait_send()
    handed(1, 4).wait_send()
    with scope("expand_own"):
        from_mate(2, 6, 1)
        expand(2, 0, 5, (xi,))
    with scope("ag2_mid"):
        ag_mid(2)
    with scope("ag2_near"):
        ag_near(2)
    near = (x1, x3)
    with scope("expand_near"):
        expand(2, 0, 3, near)
    with scope("ag2_far"):
        ag_far(2)
    with scope("expand_near"):
        expand(2, 3, 5, near)
    with scope("ag2_end"):
        ag_end(2)
    with scope("expand_far"):
        expand(2, 0, 5, (x2,))
    run(1, hb, dn, STEPS)
    with scope("norm"):
        out[...] = post_norm(2, 0.5)
    with scope("sent"):
        ag_sent(2)
        rs_sent(1)


def solution(mesh):
    n = mesh.shape["fs"]
    assert mesh.shape["grp"] % 2 == 0 and n % 2 == 0 and mesh.shape["tp"] == 8

    def per_device(x, wsw, wex, wct, wq, wk, wv, wg, wls, wle, bias, extra, gain, wo):
        T, D = x.shape
        K, F = wsw.shape
        N8 = 8 * T
        half = D // 2
        vmem = pl.BlockSpec(memory_space=pltpu.VMEM)
        anywhere = pl.BlockSpec(memory_space=pl.ANY)
        dma = pltpu.SemaphoreType.DMA
        return pl.pallas_call(
            functools.partial(kernel, n),
            out_shape=pltpu.VMEM((T, D), bf16),
            in_specs=[anywhere] * 14,
            out_specs=vmem,
            scratch_shapes=[
                pltpu.VMEM((D, 2 * F), bf16),
                pltpu.VMEM((F, D), bf16),
                pltpu.VMEM((D, 512), bf16),
                pltpu.VMEM((8 * 128, D), bf16),
                pltpu.VMEM((T, 8 * 128), bf16),
                pltpu.VMEM((3, N8, D), bf16),
                pltpu.VMEM((N8, 2 * F), f32),
                pltpu.VMEM((N8, F), bf16),
                pltpu.VMEM((2, N8 // 2, D), bf16),
                pltpu.VMEM((2, N8 // 2, D), bf16),
                pltpu.VMEM((N8 // 2, D), f32),
                pltpu.VMEM((2, 6, T, half), bf16),
                pltpu.VMEM((2, 6, T, half), bf16),
                pltpu.VMEM((T, D), f32),
                pltpu.VMEM((2 * PAD, 128), f32),
                pltpu.VMEM((2 * PAD, 128), bf16),
                pltpu.VMEM((2 * PAD, 128), f32),
                pltpu.VMEM((2 * PAD, 128), f32),
                pltpu.VMEM((9 * 128, 256), bf16),
                pltpu.VMEM((wle.shape[0], 128), f32),
                pltpu.VMEM((1, 128), f32),
                pltpu.VMEM((N8, 128), f32),
                pltpu.VMEM((N8, 128), bf16),
                pltpu.VMEM((2, wq.shape[1], K), bf16),
                pltpu.VMEM((wls.shape[1], D), bf16),
                pltpu.VMEM(wle.shape, bf16),
                pltpu.VMEM((1, bias.shape[0]), f32),
                pltpu.VMEM((extra.shape[1], extra.shape[0]), f32),
                pltpu.VMEM((1, gain.shape[0]), f32),
                dma((5, 2, 4)),
                dma((n // 2,)),
                dma((n // 2,)),
                dma((1,)),
                dma((2,)),
                dma((4, 3)),
                dma((5, 9)),
                dma((5,)),
                dma((2, CHUNKS, 4)),
                dma((2, 2)),
                dma((2,)),
                dma((2,)),
                dma((13,)),
            ],
            compiler_params=pltpu.CompilerParams(
                collective_id=0, has_side_effects=True, vmem_limit_bytes=60 * 1024 * 1024
            ),
        )(
            x, wsw, wex, wct, wq.T, wk.T, wv, wg, wls.T, wle, bias.reshape(1, -1), extra.T, gain.reshape(1, -1), wo
        )

    return jax.shard_map(
        per_device,
        mesh=mesh,
        in_specs=(
            P(("grp", "fs", "tp"), None),
            P("fs", "tp"),
            P("fs", "tp"),
            P("tp", "fs"),
            P("fs", "tp"),
            P("fs", "tp"),
            P("fs", "tp"),
            P("fs", "tp"),
            P(),
            P(None, "tp"),
            P("tp"),
            P(("grp", "fs"), "tp"),
            P(),
            P("tp", "fs"),
        ),
        out_specs=P(("grp", "fs", "tp"), None),
        check_vma=False,
    )
```
